128 devices in a mesh: sp: 16 (over z, y), tp: 8 (over x, core).
Axes of the slice: x: 4, y: 4, z: 4, core: 2. Of those that a mesh axis runs over, the one named last changes fastest.
Arguments:
- target: bfloat16 [4096, 2048], P(('sp', 'tp')), may hold values from -6 to 6
- source: bfloat16 [8192, 2048], P(('sp', 'tp')), may hold values from -6 to 6
- target_gain: bfloat16 [2, 2048], replicated, may hold values from 0.099609375 to 1.8984375
- source_gain: bfloat16 [2, 2048], replicated, may hold values from 0.099609375 to 1.8984375
- query_w: bfloat16 [2, 2048, 8192], P(None, None, 'tp'), may hold values from -0.125 to 0.125
- key_w: bfloat16 [2, 2048, 4096], P(None, None, 'tp'), may hold values from -0.125 to 0.125
- value_w: bfloat16 [2, 2048, 4096], P(None, None, 'tp'), may hold values from -0.125 to 0.125
- out_w: bfloat16 [2, 8192, 2048], P(None, 'tp'), may hold values from -0.1875 to 0.1875
- head_temp: float32 [2, 16], P(None, 'tp'), may hold values from 1.5 to 8, as said below
- final_gain: bfloat16 [2048], replicated, may hold values from 0.099609375 to 1.8984375
Outputs:
- result: float32 [4096, 2048], P(('sp', 'tp'))
The draws below stay inside these ranges and needn't reach their ends.
Inputs may be any that keep to these rules, and one draw needn't show every extreme that they name: `head_temp`: a positive scale for each head's scores.
All inputs are finite; a program needn't handle non-finite values.
Results may differ from the reference program's by a relative error of at most 0.04.
Values may be sent and summed in bfloat16 or wider, within the bound.
A program may use at most 192 MiB of HBM per device.

```python
import math
import jax
import jax.numpy as jnp
from jax import lax

D = 2048
HEAD_DIM = 512
HEADS = 16
KV_HEADS = 8
SOURCE = 8192
TARGET = 4096
N_TP = 8


def draw_head_temp(key, part):
    moderate_key = jax.random.fold_in(key, 11)
    moderate = jnp.exp(jax.random.uniform(moderate_key, (2, HEADS), jnp.float32, math.log(1.5), math.log(3.5)))
    return moderate


def block_scale(stream_key, extent, cuts, smallest, high):
    level = 1.0
    for position, parts in cuts:
        draws = jax.random.uniform(jax.random.fold_in(jax.random.fold_in(stream_key, 6), position), (parts,), jnp.float32, smallest / len(cuts), high / len(cuts))
        level = level * jnp.repeat(jnp.exp(draws), extent[position] // parts).reshape((-1,) + (1,) * (len(extent) - 1 - position))
    return level


def noise(rng, extent, width, bound, cuts=(), kind=jnp.bfloat16):
    factor_of = block_scale(rng, extent, cuts, -0.22, 0.18) if cuts else 1.0
    array = jax.random.normal(rng, extent, jnp.float32) * width * factor_of
    return jnp.minimum(jnp.maximum(array, -bound), bound).astype(kind)


def setup_inputs(seed: int = 0) -> dict:
    splits = jax.random.split(jax.random.key(seed), 11)
    target = noise(splits[0], (TARGET, D), 1.0, 6.0, ((0, 128),))
    source = noise(splits[1], (SOURCE, D), 1.0, 6.0, ((0, 128),))
    target_gain = jnp.clip(1.0 + 0.18 * jax.random.normal(splits[2], (2, D), jnp.float32), 0.099609375, 1.8984375).astype(jnp.bfloat16)
    source_gain = jnp.clip(1.0 + 0.18 * jax.random.normal(splits[3], (2, D), jnp.float32), 0.099609375, 1.8984375).astype(jnp.bfloat16)
    query_w = noise(splits[4], (2, D, HEADS * HEAD_DIM), D ** -0.5, 0.125, ((2, 8),))
    key_w = noise(splits[5], (2, D, KV_HEADS * HEAD_DIM), D ** -0.5, 0.125, ((2, 8),))
    value_w = noise(splits[6], (2, D, KV_HEADS * HEAD_DIM), D ** -0.5, 0.125, ((2, 8),))
    out_w = noise(splits[7], (2, HEADS * HEAD_DIM, D), (3.0 * (HEADS * HEAD_DIM) ** -0.5), 0.1875, ((1, 8),))
    head_temp = draw_head_temp(jax.random.fold_in(splits[10], 71), 0)
    final_gain = jnp.clip(1.0 + 0.18 * jax.random.normal(splits[9], (D,), jnp.float32), 0.099609375, 1.8984375).astype(jnp.bfloat16)
    return dict(target=target, source=source, target_gain=target_gain, source_gain=source_gain, query_w=query_w, key_w=key_w, value_w=value_w, out_w=out_w, head_temp=head_temp, final_gain=final_gain)


EPS = 1e-06

def unit_rows(matrix):
    values = matrix.astype(jnp.float32)
    return values * lax.rsqrt(lax.optimization_barrier(jnp.mean(values * values, axis=-1, keepdims=True)) + EPS)

def attend_head(queries, key_rows, value_rows, scales):
    scores = jnp.dot(queries, key_rows.T, preferred_element_type=jnp.float32) * scales
    row_max = lax.optimization_barrier(jnp.max(scores, axis=-1, keepdims=True))
    exponent = jnp.exp(scores - row_max)
    row_total = lax.optimization_barrier(jnp.sum(exponent, axis=-1, keepdims=True))
    weights = exponent.astype(jnp.bfloat16)
    summed = jnp.dot(weights, value_rows, preferred_element_type=jnp.float32)
    return (summed / row_total).astype(jnp.bfloat16)

def reference(target, source, target_gain, source_gain, query_w, key_w, value_w, out_w, head_temp, final_gain):
    unit_source = unit_rows(source)
    group_size = HEADS // KV_HEADS
    head_share = HEADS // N_TP
    hidden_state = target.astype(jnp.float32)
    for layer_index in range(2):
        normed_source = (unit_source * source_gain[layer_index].astype(jnp.float32)).astype(jnp.bfloat16)
        key_rows = jnp.dot(normed_source, key_w[layer_index], preferred_element_type=jnp.float32).astype(jnp.bfloat16)
        value_rows = jnp.dot(normed_source, value_w[layer_index], preferred_element_type=jnp.float32).astype(jnp.bfloat16)
        key_rows = key_rows.reshape(SOURCE, KV_HEADS, HEAD_DIM)
        value_rows = value_rows.reshape(SOURCE, KV_HEADS, HEAD_DIM)
        normed = (unit_rows(hidden_state) * target_gain[layer_index].astype(jnp.float32)).astype(jnp.bfloat16)
        queries = jnp.dot(normed, query_w[layer_index], preferred_element_type=jnp.float32).astype(jnp.bfloat16)
        queries = queries.reshape(TARGET, HEADS, HEAD_DIM)
        scales = head_temp[layer_index].astype(jnp.float32) * HEAD_DIM ** (-0.5)

        def one_head(head_index):
            shared_head = head_index // group_size
            return attend_head(queries[:, head_index], key_rows[:, shared_head], value_rows[:, shared_head], scales[head_index])
        heads_out = lax.map(one_head, jnp.arange(HEADS, dtype=jnp.int32))
        heads_out = heads_out.reshape(N_TP, head_share, TARGET, HEAD_DIM)
        out_parts = out_w[layer_index].reshape(N_TP, head_share, HEAD_DIM, D)

        def part_term(running, inputs):
            head_block, weights = inputs
            partial_value = jnp.einsum('htd,hde->te', head_block.astype(jnp.float32), weights.astype(jnp.float32))
            rounded = lax.optimization_barrier(partial_value.astype(jnp.bfloat16))
            return (running + rounded.astype(jnp.float32), None)
        mixed, unused = lax.scan(part_term, jnp.zeros((TARGET, D), jnp.float32), (heads_out, out_parts))
        hidden_state = hidden_state + mixed
    return unit_rows(hidden_state) * final_gain.astype(jnp.float32)
```

```python
import jax
import jax.numpy as jnp
from jax import lax
from jax.sharding import Mesh
from jax.sharding import PartitionSpec as P

HEAD_DIM = 512
EPS = 1e-06
ROWS = ("z", "y", "x", "c")
SRC_PLANE = ("y", "x", "c")
TGT_PLANE = ("z", "x", "c")
TP = ("x", "c")


def unit_rows(matrix):
    values = matrix.astype(jnp.float32)
    return values * lax.rsqrt(jnp.mean(values * values, axis=-1, keepdims=True) + EPS)


def per_device(
    target, source, target_gain, source_gain, query_w, key_w, value_w, out_w, head_temp, final_gain
):
    local_heads = query_w.shape[2] // HEAD_DIM
    src = lax.all_gather(source, SRC_PLANE, axis=0, tiled=True)
    unit_src = unit_rows(src)
    hidden = target.astype(jnp.float32)
    for l in range(2):
        normed_src = (unit_src * source_gain[l].astype(jnp.float32)).astype(jnp.bfloat16)
        k = jnp.dot(normed_src, key_w[l], preferred_element_type=jnp.float32).astype(jnp.bfloat16)
        v = jnp.dot(normed_src, value_w[l], preferred_element_type=jnp.float32).astype(jnp.bfloat16)
        normed = (unit_rows(hidden) * target_gain[l].astype(jnp.float32)).astype(jnp.bfloat16)
        full = lax.all_gather(normed, TGT_PLANE, axis=0, tiled=True)
        q = jnp.dot(full, query_w[l], preferred_element_type=jnp.float32).astype(jnp.bfloat16)
        rows = q.shape[0]
        q = q.reshape(rows, local_heads, HEAD_DIM)
        scales = head_temp[l] * HEAD_DIM ** (-0.5)
        s = jnp.einsum("thd,nd->htn", q, k, preferred_element_type=jnp.float32)
        s = s * scales[:, None, None]
        m = jnp.max(s, axis=-1)
        e = jnp.exp(s - m[..., None])
        t = jnp.sum(e, axis=-1)
        o = jnp.einsum("htn,nd->htd", e.astype(jnp.bfloat16), v, preferred_element_type=jnp.float32)
        stats = lax.all_gather(jnp.stack([m, t]), "z")
        gm = jnp.max(stats[:, 0], axis=0)
        gt = jnp.sum(stats[:, 1] * jnp.exp(stats[:, 0] - gm[None]), axis=0)
        o = o * (jnp.exp(m - gm) / gt)[..., None]
        o = o.astype(jnp.bfloat16)
        flat = o.transpose(1, 0, 2).reshape(rows, local_heads * HEAD_DIM)
        part = jnp.dot(flat, out_w[l], preferred_element_type=jnp.float32).astype(jnp.bfloat16)
        mixed = lax.psum_scatter(part, TGT_PLANE, scatter_dimension=0, tiled=True)
        hidden = hidden + mixed.astype(jnp.float32)
    return unit_rows(hidden) * final_gain.astype(jnp.float32)


def solution(mesh):
    split = Mesh(mesh.devices.reshape(4, 4, 4, 2), ROWS)
    in_specs = (
        P(ROWS, None),
        P(ROWS, None),
        P(),
        P(),
        P(None, None, TP),
        P(None, None, TP),
        P(None, None, TP),
        P(None, TP, None),
        P(None, TP),
        P(),
    )
    return jax.shard_map(
        per_device, mesh=split, in_specs=in_specs, out_specs=P(ROWS, None), check_vma=False
    )
```

```python
import functools
import math

import jax
import jax.numpy as jnp
from jax import lax
from jax.experimental import pallas as pl
from jax.experimental.pallas import tpu as pltpu
from jax.sharding import Mesh
from jax.sharding import PartitionSpec as P

HEAD_DIM = 512
D = 2048
EPS = 1e-06
ROWS = ("z", "y", "x", "c")
TP = ("x", "c")
MESH = pl.DeviceIdType.MESH
RING = 4
BF16 = jnp.bfloat16
F32 = jnp.float32
SRC_PIECE = 32
TGT_PIECE = 16
VMEM_LIMIT = 64 * 1024 * 1024 - 64 * 1024

ROUNDS = [
    [(i, r - i) for i in range(min(r, RING - 1), -1, -1) if r - i < RING]
    for r in range(2 * RING - 1)
]


def piece_no(h, i, j):
    return h * 16 + i * 4 + j


def source_slots():
    slots = {}
    for pairs in ROUNDS:
        for s in range(2):
            for h in range(2):
                for i, j in pairs:
                    slots[s, h, i, j] = len(slots)
    return slots


SRC_SLOT = source_slots()


def target_slot(s, h, i, j):
    zd, xd = (j, i) if h == 0 else (i, j)
    return (s * RING + zd) * 8 + h * 4 + xd


class Here:
    def __init__(self):
        self.at = {a: lax.axis_index(a) for a in ROWS}
        self.step = 1 - 2 * self.at["c"]

    def next(self, axis, k=1):
        return {axis: lax.rem(self.at[axis] + RING + k * self.step, RING)}

    def sibling(self):
        return {"c": 1 - self.at["c"]}


def greet(peers):
    barrier = pltpu.get_barrier_semaphore()
    for peer in peers:
        pl.semaphore_signal(barrier, inc=1, device_id=peer, device_id_type=MESH)
    pl.semaphore_wait(barrier, len(peers))


class Gather:
    def __init__(self, here, buf, rows, slot, axis, sems):
        self.here, self.buf, self.rows, self.slot, self.axis = here, buf, rows, slot, axis
        self.ring_send, self.ring_recv, self.sib_send, self.sib_recv = sems
        self.sent = []

    def ref(self, s, h, i, j):
        return self.buf.at[pl.ds(self.slot(s, h, i, j) * self.rows, self.rows), :]

    def ring(self, h, src, dst):
        first = src[1] == 0 and dst[1] == 0
        along = ("x", self.axis)[h] if first else (self.axis, "x")[h]
        n = piece_no(h, *dst)
        return pltpu.make_async_remote_copy(
            self.ref(0, h, *src), self.ref(0, h, *dst), self.ring_send.at[n], self.ring_recv.at[n],
            device_id=self.here.next(along), device_id_type=MESH,
        )

    def sib(self, h, i, j):
        n = piece_no(h, i, j)
        return pltpu.make_async_remote_copy(
            self.ref(0, h, i, j), self.ref(1, h, i, j), self.sib_send.at[n], self.sib_recv.at[n],
            device_id=self.here.sibling(), device_id_type=MESH,
        )

    def spread(self, h, i, j):
        copies = []
        if j == 0 and i < RING - 1:
            copies.append(self.ring(h, (i, 0), (i + 1, 0)))
        if j < RING - 1:
            copies.append(self.ring(h, (i, j), (i, j + 1)))
        copies.append(self.sib(h, i, j))
        for copy in copies:
            copy.start()
        self.sent += copies

    def arrive(self, h, i, j):
        src = (i, j - 1) if j > 0 else (i - 1, 0)
        self.ring(h, src, (i, j)).wait_recv()

    def arrive_sib(self, h, i, j):
        self.sib(h, i, j).wait_recv()

    def finish(self):
        for copy in self.sent:
            copy.wait_send()


def unit_times(values, gain):
    scale = lax.rsqrt(jnp.mean(values * values, axis=-1, keepdims=True) + EPS)
    return values * scale * gain.astype(F32)


def fold_gain(gain_ref, layer, w_ref):
    def body(k, carry):
        rows = pl.ds(pl.multiple_of(k * 128, 128), 128)
        g = gain_ref[layer : layer + 1, rows].astype(F32)
        g = jnp.broadcast_to(g, (128, 128)).T
        g = jnp.concatenate([g] * 4, axis=1)
        for n in range(2):
            cols = pl.ds(n * 512, 512)
            w_ref[rows, cols] = (w_ref[rows, cols].astype(F32) * g).astype(BF16)
        return carry

    lax.fori_loop(0, D // 128, body, 0)


def project_kv(src, w_ref, k_ref, v_ref, start, rows, tile):
    def body(t, carry):
        at = pl.ds(pl.multiple_of(start + t * tile, 128), tile)
        s = src[at, :]
        s32 = s.astype(F32)
        scale = lax.rsqrt(jnp.mean(s32 * s32, axis=-1, keepdims=True) + EPS)
        k = jnp.dot(s, w_ref[:, 0:512], preferred_element_type=F32)
        k_ref[at, :] = (k * scale).astype(BF16)
        v = jnp.dot(s, w_ref[:, 512:1024], preferred_element_type=F32)
        v_ref[at, :] = (v * scale).astype(BF16)
        return carry

    lax.fori_loop(0, rows // tile, body, 0)


def project_q(tgt, w_ref, q_ref, u):
    x = tgt[u * 128 : (u + 1) * 128, :]
    q = jnp.dot(x, w_ref[...], preferred_element_type=F32).astype(BF16)
    q_ref[u, 0:128, :] = q[:, 0:512]
    q_ref[u, 128:256, :] = q[:, 512:1024]


def start_all(copies):
    for copy in copies:
        copy.start()
    return copies


def wait_all(copies):
    for copy in copies:
        copy.wait()


def load_layer(layer, key_w, value_w, query_w, kv_w, q_w, sems):
    return [
        pltpu.make_async_copy(key_w.at[layer], kv_w.at[:, 0:512], sems.at[0]),
        pltpu.make_async_copy(value_w.at[layer], kv_w.at[:, 512:1024], sems.at[1]),
        pltpu.make_async_copy(query_w.at[layer], q_w, sems.at[2]),
    ]


def gather_kernel(
    target, source, target_gain, source_gain, query_w, key_w, value_w,
    src_out, k_out, v_out, q_out,
    src, tgt, kv_w, q_w, k_buf, v_buf, q_buf,
    s_ring_send, s_ring_recv, s_sib_send, s_sib_recv,
    t_ring_send, t_ring_recv, t_sib_send, t_sib_recv, load_sem, out_sem,
):
    here = Here()
    own = start_all([
        pltpu.make_async_copy(
            source.at[pl.ds(h * SRC_PIECE, SRC_PIECE), :],
            src.at[pl.ds(SRC_SLOT[0, h, 0, 0] * SRC_PIECE, SRC_PIECE), :],
            load_sem.at[3 + h],
        )
        for h in range(2)
    ])
    weights = start_all(load_layer(0, key_w, value_w, query_w, kv_w, q_w, load_sem))
    sg = Gather(here, src, SRC_PIECE, lambda *p: SRC_SLOT[p], "y", (s_ring_send, s_ring_recv, s_sib_send, s_sib_recv))
    tg = Gather(here, tgt, TGT_PIECE, target_slot, "z", (t_ring_send, t_ring_recv, t_sib_send, t_sib_recv))
    normed = unit_times(target[...].astype(F32), target_gain[0:1, :]).astype(BF16)
    tgt[0:16, :] = normed[0:16]
    tgt[64:80, :] = normed[16:32]
    greet([here.next("x", -1), here.next("y", -1), here.next("z", -1), here.sibling()])
    wait_all(own)
    for g in (sg, tg):
        for h in range(2):
            g.spread(h, 0, 0)
    wait_all(weights)
    fold_gain(source_gain, 0, kv_w)
    outs = []
    row = 0
    for r, pairs in enumerate(ROUNDS):
        if r:
            for i, j in pairs:
                for h in range(2):
                    tg.arrive(h, i, j)
                    tg.spread(h, i, j)
                    sg.arrive(h, i, j)
                    sg.spread(h, i, j)
        for i, j in pairs:
            for h in range(2):
                sg.arrive_sib(h, i, j)
                tg.arrive_sib(h, i, j)
        rows = len(pairs) * 4 * SRC_PIECE
        outs += start_all([pltpu.make_async_copy(src.at[row : row + rows], src_out.at[row : row + rows], out_sem.at[r])])
        project_kv(src, kv_w, k_buf, v_buf, row, rows, 128)
        row += rows
        if r >= 3:
            for s in range(2):
                project_q(tgt, q_w, q_buf, s * RING + r - 3)
    outs += start_all([
        pltpu.make_async_copy(k_buf, k_out, out_sem.at[7]),
        pltpu.make_async_copy(v_buf, v_out, out_sem.at[8]),
        pltpu.make_async_copy(q_buf, q_out, out_sem.at[9]),
    ])
    sg.finish()
    tg.finish()
    wait_all(outs)


def middle_kernel(
    hidden, src_in, target_gain, source_gain, query_w, key_w, value_w,
    k_out, v_out, q_out,
    src, tgt, kv_w, q_w, k_buf, v_buf, q_buf,
    t_ring_send, t_ring_recv, t_sib_send, t_sib_recv, load_sem, out_sem,
):
    here = Here()
    loads = start_all(load_layer(1, key_w, value_w, query_w, kv_w, q_w, load_sem))
    loads += start_all([pltpu.make_async_copy(src_in, src, load_sem.at[3])])
    tg = Gather(here, tgt, TGT_PIECE, target_slot, "z", (t_ring_send, t_ring_recv, t_sib_send, t_sib_recv))
    normed = unit_times(hidden[...], target_gain[1:2, :]).astype(BF16)
    tgt[0:16, :] = normed[0:16]
    tgt[64:80, :] = normed[16:32]
    greet([here.next("x", -1), here.next("z", -1), here.sibling()])
    for h in range(2):
        tg.spread(h, 0, 0)
    wait_all(loads)
    fold_gain(source_gain, 1, kv_w)
    row = 0
    shares = [384, 384, 384, 384, 256, 256, 0]
    for r, pairs in enumerate(ROUNDS):
        if r:
            for i, j in pairs:
                for h in range(2):
                    tg.arrive(h, i, j)
                    tg.spread(h, i, j)
        if shares[r]:
            project_kv(src, kv_w, k_buf, v_buf, row, shares[r], 128)
        row += shares[r]
        for i, j in pairs:
            for h in range(2):
                tg.arrive_sib(h, i, j)
        if r >= 3:
            for s in range(2):
                project_q(tgt, q_w, q_buf, s * RING + r - 3)
    outs = start_all([
        pltpu.make_async_copy(k_buf, k_out, out_sem.at[0]),
        pltpu.make_async_copy(v_buf, v_out, out_sem.at[1]),
        pltpu.make_async_copy(q_buf, q_out, out_sem.at[2]),
    ])
    tg.finish()
    wait_all(outs)


def attention_kernel(
    layer, last,
    hidden, head_temp, final_gain, q_in, k_in, v_in, out_w,
    result,
    q_buf, k_buf, v_buf, w_buf, e_buf, o_buf, p_buf, sib_out, sib_in, ring_out, ring_in, st_own, st_in,
    load_sem, st_send, st_recv, sib_send, sib_recv, ring_send, ring_recv,
):
    here = Here()
    qk = start_all([
        pltpu.make_async_copy(k_in, k_buf, load_sem.at[0]),
        pltpu.make_async_copy(q_in, q_buf, load_sem.at[1]),
    ])
    late = start_all([
        pltpu.make_async_copy(v_in, v_buf, load_sem.at[2]),
        pltpu.make_async_copy(out_w.at[layer], w_buf, load_sem.at[3]),
    ])
    greet(
        [here.next("z", k) for k in range(1, RING)] + [here.next("x", 1), here.sibling()]
    )
    log2e = 1.0 / math.log(2.0)
    upper = lax.broadcasted_iota(jnp.int32, (256, 1), 0) < 128
    scale = jnp.where(upper, head_temp[layer, 0], head_temp[layer, 1]) * (HEAD_DIM ** (-0.5) * log2e)
    pending = []

    def stats_copy(k):
        return pltpu.make_async_remote_copy(
            st_own, st_in.at[k - 1], st_send.at[k - 1], st_recv.at[k - 1],
            device_id=here.next("z", k), device_id_type=MESH,
        )

    def score(u, carry):
        scores = lax.dot_general(
            q_buf[u], k_buf[...], (((1,), (1,)), ((), ())), preferred_element_type=F32
        )
        top = jnp.max(scores, axis=-1, keepdims=True)
        expo = jnp.exp2((scores - top) * scale)
        total = jnp.sum(expo, axis=-1, keepdims=True)
        e_buf[u] = expo.astype(BF16)
        lane = lax.broadcasted_iota(jnp.int32, (256, 128), 1)
        both = jnp.where(lane == 0, top * scale, total)
        st_own[u] = both.T[0:8, :]
        return carry

    def attend(zd):
        def body(s, carry):
            u = s * RING + zd
            o_buf[u] = jnp.dot(e_buf[u], v_buf[...], preferred_element_type=F32)
            return carry

        lax.fori_loop(0, 2, body, 0)

    def sib_copy(zd):
        return pltpu.make_async_remote_copy(
            sib_out.at[zd], sib_in.at[zd], sib_send.at[zd], sib_recv.at[zd],
            device_id=here.sibling(), device_id_type=MESH,
        )

    def mix(zd):
        for s in range(1, -1, -1):
            u = s * RING + zd
            own = st_own[u]
            others = []
            for k in range(1, RING):
                there = (zd - k) % RING if s == 0 else (zd + k) % RING
                others.append(st_in[k - 1, s * RING + there])
            top = own[0:1]
            for o in others:
                top = jnp.maximum(top, o[0:1])
            total = own[1:2] * jnp.exp2(own[0:1] - top)
            for o in others:
                total += o[1:2] * jnp.exp2(o[0:1] - top)
            factor = jnp.exp2(own[0:1] - top) / total
            factor = jnp.broadcast_to(factor, (128, 256)).T
            factor = jnp.concatenate([factor] * 4, axis=1)
            att = (o_buf[u] * factor).astype(BF16)
            flat = jnp.concatenate([att[0:128], att[128:256]], axis=1)
            part = jnp.dot(flat, w_buf[...], preferred_element_type=F32)
            if s == 1:
                sib_out[zd] = part.astype(BF16)
                copy = sib_copy(zd)
                copy.start()
                pending.append(copy)
            else:
                p_buf[zd] = part

    def ring_copy(h, i, j):
        along = (("x", "z")[h] if j == 0 else ("z", "x")[h])
        n = piece_no(h, i, j)
        return pltpu.make_async_remote_copy(
            ring_out.at[n], ring_in.at[n], ring_send.at[n], ring_recv.at[n],
            device_id=here.next(along, -1), device_id_type=MESH,
        )

    def collect(h, i, j):
        zd, xd = (j, i) if h == 0 else (i, j)
        at = pl.ds((h * 4 + xd) * 16, 16)
        value = p_buf[zd, at, :] + sib_in[zd, at, :].astype(F32)
        if j < RING - 1:
            ring_copy(h, i, j + 1).wait_recv()
            value += ring_in[piece_no(h, i, j + 1)].astype(F32)
        if j == 0 and i < RING - 1:
            ring_copy(h, i + 1, 0).wait_recv()
            value += ring_in[piece_no(h, i + 1, 0)].astype(F32)
        return value

    def pass_on(h, i, j):
        ring_out[piece_no(h, i, j)] = collect(h, i, j).astype(BF16)
        copy = ring_copy(h, i, j)
        copy.start()
        pending.append(copy)

    wait_all(qk)
    lax.fori_loop(0, 8, score, 0)
    for k in range(1, RING):
        copy = stats_copy(k)
        copy.start()
        pending.append(copy)
    wait_all(late)
    attend(3)
    attend(2)
    for k in range(1, RING):
        stats_copy(k).wait_recv()
    mix(3)
    attend(1)
    sib_copy(3).wait_recv()
    for i in (3, 2, 1, 0):
        pass_on(0, i, 3)
    pass_on(1, 3, 3)
    mix(2)
    attend(0)
    sib_copy(2).wait_recv()
    for i in (3, 2, 1, 0):
        pass_on(0, i, 2)
    pass_on(1, 2, 3)
    pass_on(1, 3, 2)
    mix(1)
    sib_copy(1).wait_recv()
    for i in (3, 2, 1, 0):
        pass_on(0, i, 1)
    pass_on(1, 1, 3)
    pass_on(1, 2, 2)
    pass_on(1, 3, 1)
    mix(0)
    sib_copy(0).wait_recv()
    pass_on(1, 0, 3)
    pass_on(0, 3, 0)
    pass_on(1, 1, 2)
    pass_on(1, 2, 1)
    pass_on(1, 3, 0)
    pass_on(1, 0, 2)
    pass_on(0, 2, 0)
    pass_on(1, 1, 1)
    pass_on(1, 2, 0)
    pass_on(1, 0, 1)
    pass_on(0, 1, 0)
    pass_on(1, 1, 0)
    for h in range(2):
        at = slice(h * 16, h * 16 + 16)
        value = hidden[at, :].astype(F32) + collect(h, 0, 0)
        if last:
            value = unit_times(value, final_gain[...])
        result[at, :] = value
    for copy in pending:
        copy.wait_send()


def vmem(*shape, dtype=BF16):
    return pltpu.VMEM(shape, dtype)


ANY = pl.BlockSpec(memory_space=pl.ANY)
INV = pl.BlockSpec(memory_space=pltpu.VMEM)
DMA = pltpu.SemaphoreType.DMA


def params(collective_id):
    return pltpu.CompilerParams(
        collective_id=collective_id, has_side_effects=True, vmem_limit_bytes=VMEM_LIMIT
    )


KV_SHAPE = jax.ShapeDtypeStruct((2048, HEAD_DIM), BF16)
Q_SHAPE = jax.ShapeDtypeStruct((8, 256, HEAD_DIM), BF16)
SRC_SHAPE = jax.ShapeDtypeStruct((2048, D), BF16)
PROJECT_SCRATCH = [
    vmem(2048, D), vmem(1024, D), vmem(D, 1024), vmem(D, 1024),
    vmem(2048, HEAD_DIM), vmem(2048, HEAD_DIM), vmem(8, 256, HEAD_DIM),
]


def per_device(
    target, source, target_gain, source_gain, query_w, key_w, value_w, out_w, head_temp, final_gain
):
    src_all, k, v, q = pl.pallas_call(
        gather_kernel,
        out_shape=[SRC_SHAPE, KV_SHAPE, KV_SHAPE, Q_SHAPE],
        in_specs=[INV, ANY, INV, INV, ANY, ANY, ANY],
        out_specs=[ANY] * 4,
        scratch_shapes=PROJECT_SCRATCH + [DMA((32,))] * 8 + [DMA((5,)), DMA((10,))],
        compiler_params=params(0),
        name="gather0",
    )(target, source, target_gain, source_gain, query_w, key_w, value_w)

    def attend(layer, hidden, q, k, v):
        return pl.pallas_call(
            functools.partial(attention_kernel, layer, layer == 1),
            out_shape=jax.ShapeDtypeStruct((32, D), F32),
            in_specs=[INV, pl.BlockSpec(memory_space=pltpu.SMEM), INV, ANY, ANY, ANY, ANY],
            out_specs=INV,
            scratch_shapes=[
                vmem(8, 256, HEAD_DIM), vmem(2048, HEAD_DIM), vmem(2048, HEAD_DIM), vmem(1024, D),
                vmem(8, 256, 2048), vmem(8, 256, HEAD_DIM, dtype=F32), vmem(4, 128, D, dtype=F32),
                vmem(4, 128, D), vmem(4, 128, D), vmem(32, 16, D), vmem(32, 16, D),
                vmem(8, 8, 256, dtype=F32), vmem(3, 8, 8, 256, dtype=F32),
                DMA((4,)), DMA((3,)), DMA((3,)), DMA((4,)), DMA((4,)), DMA((32,)), DMA((32,)),
            ],
            compiler_params=params(1 + layer),
            name=f"attend{layer}",
        )(hidden, head_temp, final_gain.reshape(1, D), q, k, v, out_w)

    hidden = attend(0, target, q, k, v)
    k, v, q = pl.pallas_call(
        middle_kernel,
        out_shape=[KV_SHAPE, KV_SHAPE, Q_SHAPE],
        in_specs=[INV, ANY, INV, INV, ANY, ANY, ANY],
        out_specs=[ANY] * 3,
        scratch_shapes=PROJECT_SCRATCH + [DMA((32,))] * 4 + [DMA((4,)), DMA((3,))],
        compiler_params=params(3),
        name="gather1",
    )(hidden, src_all, target_gain, source_gain, query_w, key_w, value_w)
    return attend(1, hidden, q, k, v)


def solution(mesh):
    split = Mesh(mesh.devices.reshape(4, 4, 4, 2), ROWS)
    in_specs = (
        P(ROWS, None),
        P(ROWS, None),
        P(),
        P(),
        P(None, None, TP),
        P(None, None, TP),
        P(None, None, TP),
        P(None, TP, None),
        P(None, TP),
        P(),
    )
    return jax.shard_map(
        per_device, mesh=split, in_specs=in_specs, out_specs=P(ROWS, None), check_vma=False
    )
```

```python
import functools
import math

import jax
import jax.numpy as jnp
from jax import lax
from jax.experimental import pallas as pl
from jax.experimental.pallas import tpu as pltpu
from jax.sharding import Mesh
from jax.sharding import PartitionSpec as P

HEAD_DIM = 512
D = 2048
EPS = 1e-06
ROWS = ("z", "y", "x", "c")
TP = ("x", "c")
MESH = pl.DeviceIdType.MESH
RING = 4
BF16 = jnp.bfloat16
F32 = jnp.float32
SRC_PIECE = 32
TGT_PIECE = 16
VMEM_LIMIT = 64 * 1024 * 1024 - 64 * 1024
VIA = (1, -1)
AWAY = (0, 1, 2, 1)
ROUNDS = [
    sorted(
        [(i, j) for i in range(RING) for j in range(RING) if AWAY[i] + AWAY[j] == r],
        key=lambda p: (p[1] != 0, p),
    )
    for r in range(5)
]


def piece_no(h, i, j):
    return h * 16 + i * 4 + j


def source_slots():
    slots = {}
    for pairs in ROUNDS:
        for s in range(2):
            for h in range(2):
                for i, j in pairs:
                    slots[s, h, i, j] = len(slots)
    return slots


SRC_SLOT = source_slots()


def line_sends(h, o):
    if o == 0:
        return [(1, 3), (-1, 1)]
    if o == 1 and VIA[h] == 1:
        return [(-1, 2)]
    if o == 3 and VIA[h] == -1:
        return [(1, 2)]
    return []


def line_up(h, o):
    if o == 2:
        return (1, 1) if VIA[h] == 1 else (-1, 3)
    return (1, 0) if o == 1 else (-1, 0)


class Here:
    def __init__(self):
        self.at = {a: lax.axis_index(a) for a in ROWS}
        self.step = 1 - 2 * self.at["c"]

    def next(self, axis, k=1):
        return {axis: lax.rem(self.at[axis] + RING + k * self.step, RING)}

    def sibling(self):
        return {"c": 1 - self.at["c"]}


def greet(peers):
    barrier = pltpu.get_barrier_semaphore()
    for peer in peers:
        pl.semaphore_signal(barrier, inc=1, device_id=peer, device_id_type=MESH)
    pl.semaphore_wait(barrier, len(peers))


class Gather:
    def __init__(self, here, buf, rows, slot, order, sems):
        self.here, self.buf, self.rows, self.slot, self.order = here, buf, rows, slot, order
        self.ring_send, self.ring_recv, self.sib_send, self.sib_recv = sems
        self.sent = []

    def ref(self, s, h, i, j):
        return self.buf.at[pl.ds(self.slot(s, h, i, j) * self.rows, self.rows), :]

    def ring(self, h, src, dst, axis, way):
        n = piece_no(h, *dst)
        return pltpu.make_async_remote_copy(
            self.ref(0, h, *src), self.ref(0, h, *dst), self.ring_send.at[n], self.ring_recv.at[n],
            device_id=self.here.next(axis, way), device_id_type=MESH,
        )

    def sib(self, h, i, j):
        n = piece_no(h, i, j)
        return pltpu.make_async_remote_copy(
            self.ref(0, h, i, j), self.ref(1, h, i, j), self.sib_send.at[n], self.sib_recv.at[n],
            device_id=self.here.sibling(), device_id_type=MESH,
        )

    def spread(self, h, i, j):
        copies = []
        first, second = self.order[h]
        if j == 0:
            copies += [self.ring(h, (i, 0), (o, 0), first, way) for way, o in line_sends(h, i)]
        copies += [self.ring(h, (i, j), (i, o), second, way) for way, o in line_sends(h, j)]
        copies.append(self.sib(h, i, j))
        self.sent += start_all(copies)

    def arrive(self, h, i, j):
        self.ring(h, (0, 0), (i, j), "x", 1).wait_recv()

    def arrive_sib(self, h, i, j):
        self.sib(h, i, j).wait_recv()

    def finish(self):
        for copy in self.sent:
            copy.wait_send()


def target_slot(order):
    def slot(s, h, i, j):
        zd, xd = (j, i) if order[h][0] == "x" else (i, j)
        return (zd * 2 + s) * 8 + h * 4 + xd

    return slot


XX = (("x", "z"), ("x", "z"))
XZ = (("x", "z"), ("z", "x"))
XY = (("x", "y"), ("y", "x"))


def unit_times(values, gain):
    scale = lax.rsqrt(jnp.mean(values * values, axis=-1, keepdims=True) + EPS)
    return values * scale * gain.astype(F32)


def fold_gain(gain_ref, layer, w_ref):
    def body(k, carry):
        rows = pl.ds(pl.multiple_of(k * 128, 128), 128)
        g = gain_ref[layer : layer + 1, rows].astype(F32)
        g = jnp.broadcast_to(g, (128, 128)).T
        g = jnp.concatenate([g] * 4, axis=1)
        for n in range(2):
            cols = pl.ds(n * 512, 512)
            w_ref[rows, cols] = (w_ref[rows, cols].astype(F32) * g).astype(BF16)
        return carry

    lax.fori_loop(0, D // 128, body, 0)


def project_kv(src, w_ref, kv_ref, start, rows):
    s32 = src[start : start + rows, :].astype(F32)
    scale = lax.rsqrt(jnp.mean(s32 * s32, axis=-1, keepdims=True) + EPS)

    def body(n, carry):
        cols = pl.ds(pl.multiple_of(n * 256, 256), 256)
        kv = jnp.dot(src[start : start + rows, :], w_ref[:, cols], preferred_element_type=F32)
        kv_ref[start : start + rows, cols] = (kv * scale).astype(BF16)
        return carry

    lax.fori_loop(0, 4, body, 0)


def project_q(tgt, w_ref, q_ref, o):
    def body(n, carry):
        cols = pl.ds(pl.multiple_of(n * 512, 512), 512)
        rows = pl.ds(pl.multiple_of(n * 256, 256), 256)
        q = jnp.dot(tgt[o * 256 : o * 256 + 256, :], w_ref[:, cols], preferred_element_type=F32)
        q_ref[o, rows, :] = q.astype(BF16)
        return carry

    lax.fori_loop(0, 2, body, 0)


def start_all(copies):
    for copy in copies:
        copy.start()
    return copies


def wait_all(copies):
    for copy in copies:
        copy.wait()


def load_layer(layer, key_w, value_w, query_w, kv_w, q_w, sems):
    return [
        pltpu.make_async_copy(key_w.at[layer], kv_w.at[:, 0:512], sems.at[0]),
        pltpu.make_async_copy(value_w.at[layer], kv_w.at[:, 512:1024], sems.at[1]),
        pltpu.make_async_copy(query_w.at[layer], q_w, sems.at[2]),
    ]


def place_target(tgt, slot, normed):
    for h in range(2):
        row = slot(0, h, 0, 0) * TGT_PIECE
        tgt[row : row + 16, :] = normed[h * 16 : h * 16 + 16]


def gather_kernel(
    target, source, target_gain, source_gain, query_w, key_w, value_w,
    src_out, kv_out, q_out,
    src, tgt, kv_w, q_w, kv_buf, q_buf,
    s_ring_send, s_ring_recv, s_sib_send, s_sib_recv,
    t_ring_send, t_ring_recv, t_sib_send, t_sib_recv, load_sem, out_sem,
):
    here = Here()
    own = start_all([
        pltpu.make_async_copy(
            source.at[pl.ds(h * SRC_PIECE, SRC_PIECE), :],
            src.at[pl.ds(SRC_SLOT[0, h, 0, 0] * SRC_PIECE, SRC_PIECE), :],
            load_sem.at[3 + h],
        )
        for h in range(2)
    ])
    weights = start_all(load_layer(0, key_w, value_w, query_w, kv_w, q_w, load_sem))
    slot = target_slot(XX)
    sg = Gather(here, src, SRC_PIECE, lambda *p: SRC_SLOT[p], XY, (s_ring_send, s_ring_recv, s_sib_send, s_sib_recv))
    tg = Gather(here, tgt, TGT_PIECE, slot, XX, (t_ring_send, t_ring_recv, t_sib_send, t_sib_recv))
    place_target(tgt, slot, unit_times(target[...].astype(F32), target_gain[0:1, :]).astype(BF16))
    greet([here.next(a, k) for a in "xyz" for k in (1, -1)] + [here.sibling()])
    wait_all(own)
    for g in (sg, tg):
        for h in range(2):
            g.spread(h, 0, 0)
    outs = []

    def emit(copies):
        outs.extend(start_all(copies))

    def kv_rows(start, rows, n):
        emit([pltpu.make_async_copy(src.at[start : start + rows], src_out.at[start : start + rows], out_sem.at[n])])
        project_kv(src, kv_w, kv_buf, start, rows)
        emit([pltpu.make_async_copy(kv_buf.at[start : start + rows], kv_out.at[start : start + rows], out_sem.at[4 + n])])

    def q_rows(o):
        project_q(tgt, q_w, q_buf, o)
        emit([pltpu.make_async_copy(q_buf.at[o], q_out.at[o], out_sem.at[8 + o])])

    def arrive_sib(r):
        for i, j in ROUNDS[r]:
            for h in range(2):
                tg.arrive_sib(h, i, j)
                sg.arrive_sib(h, i, j)

    for r in range(1, 5):
        for i, j in ROUNDS[r]:
            for h in range(2):
                tg.arrive(h, i, j)
                tg.spread(h, i, j)
                sg.arrive(h, i, j)
                sg.spread(h, i, j)
        arrive_sib(r - 1)
        if r == 1:
            wait_all(weights)
            fold_gain(source_gain, 0, kv_w)
        if r == 2:
            kv_rows(0, 640, 0)
        if r == 3:
            kv_rows(640, 384, 1)
            kv_rows(1024, 384, 2)
            q_rows(0)
        if r == 4:
            q_rows(1)
            q_rows(3)
    arrive_sib(4)
    kv_rows(1408, 640, 3)
    q_rows(2)
    sg.finish()
    tg.finish()
    wait_all(outs)


def middle_kernel(
    hidden, src_in, target_gain, source_gain, query_w, key_w, value_w,
    kv_out, q_out,
    src, tgt, kv_w, q_w, kv_buf, q_buf,
    t_ring_send, t_ring_recv, t_sib_send, t_sib_recv, load_sem, out_sem,
):
    here = Here()
    loads = start_all(load_layer(1, key_w, value_w, query_w, kv_w, q_w, load_sem))
    src_load = pltpu.make_async_copy(src_in, src, load_sem.at[3])
    src_load.start()
    slot = target_slot(XZ)
    tg = Gather(here, tgt, TGT_PIECE, slot, XZ, (t_ring_send, t_ring_recv, t_sib_send, t_sib_recv))
    place_target(tgt, slot, unit_times(hidden[...], target_gain[1:2, :]).astype(BF16))
    greet([here.next(a, k) for a in "xz" for k in (1, -1)] + [here.sibling()])
    for h in range(2):
        tg.spread(h, 0, 0)
    outs = []

    def emit(copies):
        outs.extend(start_all(copies))

    def kv_rows(n):
        at = slice(n * 512, n * 512 + 512)
        project_kv(src, kv_w, kv_buf, n * 512, 512)
        emit([pltpu.make_async_copy(kv_buf.at[at], kv_out.at[at], out_sem.at[n])])

    def q_rows(o):
        project_q(tgt, q_w, q_buf, o)
        emit([pltpu.make_async_copy(q_buf.at[o], q_out.at[o], out_sem.at[4 + o])])

    def arrive_sib(r):
        for i, j in ROUNDS[r]:
            for h in range(2):
                tg.arrive_sib(h, i, j)

    wait_all(loads)
    fold_gain(source_gain, 1, kv_w)
    for r in range(1, 5):
        for i, j in ROUNDS[r]:
            for h in range(2):
                tg.arrive(h, i, j)
                tg.spread(h, i, j)
        arrive_sib(r - 1)
        if r == 1:
            src_load.wait()
            kv_rows(0)
        if r == 2:
            kv_rows(1)
        if r == 3:
            kv_rows(2)
            q_rows(0)
        if r == 4:
            q_rows(1)
            q_rows(3)
    kv_rows(3)
    arrive_sib(4)
    q_rows(2)
    tg.finish()
    wait_all(outs)


def attention_kernel(
    layer, last,
    hidden, head_temp, final_gain, q_in, kv_in, out_w,
    result,
    q_buf, k_buf, v_buf, w_buf, e_buf, o_buf, p_buf, att, att_out, ring_out, ring_in, st_own, st_in,
    load_sem, st_send, st_recv, sib_send, sib_recv, ring_send, ring_recv,
):
    here = Here()
    qk = start_all([
        pltpu.make_async_copy(kv_in.at[:, 0:512], k_buf, load_sem.at[0]),
        pltpu.make_async_copy(q_in, q_buf, load_sem.at[1]),
    ])
    late = start_all([
        pltpu.make_async_copy(kv_in.at[:, 512:1024], v_buf, load_sem.at[2]),
        pltpu.make_async_copy(out_w.at[layer], w_buf.at[0:1024], load_sem.at[3]),
    ])
    greet(
        [here.next("z", k) for k in range(1, RING)] + [here.next("x", 1), here.next("x", -1), here.sibling()]
    )
    w_copy = pltpu.make_async_remote_copy(
        out_w.at[layer], w_buf.at[1024:2048], sib_send.at[4], sib_recv.at[4],
        device_id=here.sibling(), device_id_type=MESH,
    )
    w_copy.start()
    pending = [w_copy]
    log2e = 1.0 / math.log(2.0)
    upper = lax.broadcasted_iota(jnp.int32, (512, 1), 0) < 256
    scale = jnp.where(upper, head_temp[layer, 0], head_temp[layer, 1]) * (HEAD_DIM ** (-0.5) * log2e)

    def stats_copy(k):
        return pltpu.make_async_remote_copy(
            st_own, st_in.at[k - 1], st_send.at[k - 1], st_recv.at[k - 1],
            device_id=here.next("z", k), device_id_type=MESH,
        )

    def score(o, carry):
        scores = lax.dot_general(
            q_buf[o], k_buf[...], (((1,), (1,)), ((), ())), preferred_element_type=F32
        )
        top = jnp.max(scores, axis=-1, keepdims=True)
        expo = jnp.exp2((scores - top) * scale)
        total = jnp.sum(expo, axis=-1, keepdims=True)
        e_buf[o] = expo.astype(BF16)
        lane = lax.broadcasted_iota(jnp.int32, (512, 128), 1)
        both = jnp.where(lane == 0, top * scale, total)
        st_own[o] = both.T[0:8, :]
        return carry

    def attend(o):
        o_buf[o] = jnp.dot(e_buf[o], v_buf[...], preferred_element_type=F32)

    def att_copy(o):
        return pltpu.make_async_remote_copy(
            att_out.at[o], att.at[o, :, 1024:2048], sib_send.at[o], sib_recv.at[o],
            device_id=here.sibling(), device_id_type=MESH,
        )

    def peer_stats(k, o, what):
        parts = []
        for n in range(4):
            there = (o + k) % RING if n % 2 == 0 else (o - k) % RING
            parts.append(st_in[k - 1, there, what : what + 1, n * 128 : n * 128 + 128])
        return jnp.concatenate(parts, axis=1)

    def weigh(o):
        own = st_own[o]
        tops = [own[0:1]] + [peer_stats(k, o, 0) for k in range(1, RING)]
        totals = [own[1:2]] + [peer_stats(k, o, 1) for k in range(1, RING)]
        top = functools.reduce(jnp.maximum, tops)
        total = sum(t * jnp.exp2(m - top) for m, t in zip(tops, totals))
        factor = jnp.exp2(own[0:1] - top) / total
        factor = jnp.broadcast_to(factor, (128, 512)).T
        factor = jnp.concatenate([factor] * 4, axis=1)
        rows = (o_buf[o] * factor).astype(BF16)
        for head in range(2):
            cols = slice(head * 512, head * 512 + 512)
            att_out[o, :, cols] = rows[head * 256 + 128 : head * 256 + 256]
            att[o, :, cols] = rows[head * 256 : head * 256 + 128]
        pending.extend(start_all([att_copy(o)]))

    def mix(o):
        att_copy(o).wait_recv()

        def body(n, carry):
            cols = pl.ds(pl.multiple_of(n * 512, 512), 512)
            p_buf[o, :, cols] = jnp.dot(att[o], w_buf[:, cols], preferred_element_type=F32)
            return carry

        lax.fori_loop(0, 4, body, 0)

    def ring_copy(h, i, j):
        axis, way = (XZ[h][1], line_up(h, j)[0]) if j else (XZ[h][0], line_up(h, i)[0])
        n = piece_no(h, i, j)
        return pltpu.make_async_remote_copy(
            ring_out.at[n], ring_in.at[n], ring_send.at[n], ring_recv.at[n],
            device_id=here.next(axis, way), device_id_type=MESH,
        )

    def collect(h, i, j):
        zd, xd = (j, i) if h == 0 else (i, j)
        at = pl.ds((h * 4 + xd) * 16, 16)
        value = p_buf[zd, at, :]
        below = [(i, o) for way, o in line_sends(h, j)]
        if j == 0:
            below += [(o, 0) for way, o in line_sends(h, i)]
        for label in below:
            ring_copy(h, *label).wait_recv()
            value += ring_in[piece_no(h, *label)].astype(F32)
        return value

    def pass_on(h, i, j):
        ring_out[piece_no(h, i, j)] = collect(h, i, j).astype(BF16)
        pending.extend(start_all([ring_copy(h, i, j)]))

    def pass_unit(o, xds, halves=(0, 1)):
        for xd in xds:
            for h in halves:
                pass_on(h, *((xd, o) if h == 0 else (o, xd)))

    wait_all(qk)
    lax.fori_loop(0, 4, score, 0)
    for k in range(1, RING):
        pending.extend(start_all([stats_copy(k)]))
    wait_all(late)
    attend(2)
    attend(1)
    for k in range(1, RING):
        stats_copy(k).wait_recv()
    weigh(2)
    weigh(1)
    attend(3)
    weigh(3)
    w_copy.wait_recv()
    mix(2)
    pass_unit(2, (2, 1, 3, 0), (0,))
    pass_unit(2, (2,), (1,))
    attend(0)
    weigh(0)
    mix(1)
    pass_unit(2, (1, 3), (1,))
    pass_unit(1, (2, 1, 3, 0), (0,))
    pass_unit(1, (2,), (1,))
    mix(3)
    pass_unit(2, (0,), (1,))
    pass_unit(3, (2, 1, 3, 0), (0,))
    pass_unit(3, (2,), (1,))
    pass_unit(1, (1, 3), (1,))
    mix(0)
    pass_unit(0, (2,), (0, 1))
    pass_unit(3, (1, 3), (1,))
    pass_unit(1, (0,), (1,))
    pass_unit(3, (0,), (1,))
    pass_unit(0, (1, 3), (1, 0))
    for h in range(2):
        at = slice(h * 16, h * 16 + 16)
        value = hidden[at, :].astype(F32) + collect(h, 0, 0)
        if last:
            value = unit_times(value, final_gain[...])
        result[at, :] = value
    for copy in pending:
        copy.wait_send()


def vmem(*shape, dtype=BF16):
    return pltpu.VMEM(shape, dtype)


ANY = pl.BlockSpec(memory_space=pl.ANY)
INV = pl.BlockSpec(memory_space=pltpu.VMEM)
DMA = pltpu.SemaphoreType.DMA


def params(collective_id):
    return pltpu.CompilerParams(
        collective_id=collective_id, has_side_effects=True, vmem_limit_bytes=VMEM_LIMIT
    )


KV_SHAPE = jax.ShapeDtypeStruct((2048, 1024), BF16)
Q_SHAPE = jax.ShapeDtypeStruct((4, 512, HEAD_DIM), BF16)
SRC_SHAPE = jax.ShapeDtypeStruct((2048, D), BF16)
PROJECT_SCRATCH = [
    vmem(2048, D), vmem(1024, D), vmem(D, 1024), vmem(D, 1024), vmem(2048, 1024), vmem(4, 512, HEAD_DIM),
]


def per_device(
    target, source, target_gain, source_gain, query_w, key_w, value_w, out_w, head_temp, final_gain
):
    src_all, kv, q = pl.pallas_call(
        gather_kernel,
        out_shape=[SRC_SHAPE, KV_SHAPE, Q_SHAPE],
        in_specs=[INV, ANY, INV, INV, ANY, ANY, ANY],
        out_specs=[ANY] * 3,
        scratch_shapes=PROJECT_SCRATCH + [DMA((32,))] * 8 + [DMA((5,)), DMA((12,))],
        compiler_params=params(0),
        name="gather0",
    )(target, source, target_gain, source_gain, query_w, key_w, value_w)

    def attend(layer, hidden, q, kv):
        return pl.pallas_call(
            functools.partial(attention_kernel, layer, layer == 1),
            out_shape=jax.ShapeDtypeStruct((32, D), F32),
            in_specs=[INV, pl.BlockSpec(memory_space=pltpu.SMEM), INV, ANY, ANY, ANY],
            out_specs=INV,
            scratch_shapes=[
                vmem(4, 512, HEAD_DIM), vmem(2048, HEAD_DIM), vmem(2048, HEAD_DIM), vmem(2048, D),
                vmem(4, 512, 2048), vmem(4, 512, HEAD_DIM, dtype=F32), vmem(4, 128, D, dtype=F32),
                vmem(4, 128, D), vmem(4, 128, 1024), vmem(32, 16, D), vmem(32, 16, D),
                vmem(4, 8, 512, dtype=F32), vmem(3, 4, 8, 512, dtype=F32),
                DMA((4,)), DMA((3,)), DMA((3,)), DMA((5,)), DMA((5,)), DMA((32,)), DMA((32,)),
            ],
            compiler_params=params(1 + layer),
            name=f"attend{layer}",
        )(hidden, head_temp, final_gain.reshape(1, D), q, kv, out_w)

    hidden = attend(0, target, q, kv)
    kv, q = pl.pallas_call(
        middle_kernel,
        out_shape=[KV_SHAPE, Q_SHAPE],
        in_specs=[INV, ANY, INV, INV, ANY, ANY, ANY],
        out_specs=[ANY] * 2,
        scratch_shapes=PROJECT_SCRATCH + [DMA((32,))] * 4 + [DMA((4,)), DMA((8,))],
        compiler_params=params(3),
        name="gather1",
    )(hidden, src_all, target_gain, source_gain, query_w, key_w, value_w)
    return attend(1, hidden, q, kv)


def solution(mesh):
    split = Mesh(mesh.devices.reshape(4, 4, 4, 2), ROWS)
    in_specs = (
        P(ROWS, None),
        P(ROWS, None),
        P(),
        P(),
        P(None, None, TP),
        P(None, None, TP),
        P(None, None, TP),
        P(None, TP, None),
        P(None, TP),
        P(),
    )
    return jax.shard_map(
        per_device, mesh=split, in_specs=in_specs, out_specs=P(ROWS, None), check_vma=False
    )
```

```python
import functools
import math

import jax
import jax.numpy as jnp
from jax import lax
from jax.experimental import pallas as pl
from jax.experimental.pallas import tpu as pltpu
from jax.sharding import Mesh
from jax.sharding import PartitionSpec as P

HEAD_DIM = 512
D = 2048
EPS = 1e-06
ROWS = ("z", "y", "x", "c")
TP = ("x", "c")
MESH = pl.DeviceIdType.MESH
RING = 4
BF16 = jnp.bfloat16
F32 = jnp.float32
GROUPS = 4
SRC_PIECE = 16
TGT_PIECE = 16
VMEM_LIMIT = 64 * 1024 * 1024 - 64 * 1024
VIA = (1, -1, -1, 1)
AWAY = (0, 1, 2, 1)
XX = (("x", "z"),) * GROUPS
XZ = (("x", "z"), ("z", "x")) * 2
XY = (("x", "y"), ("y", "x")) * 2
ROUNDS = [
    sorted(
        [(i, j) for i in range(RING) for j in range(RING) if AWAY[i] + AWAY[j] == r],
        key=lambda p: (p[1] != 0, p),
    )
    for r in range(5)
]


def piece_no(h, i, j):
    return h * 16 + i * 4 + j


def source_slots():
    slots = {}
    for pairs in ROUNDS:
        for s in range(2):
            for h in range(GROUPS):
                for i, j in pairs:
                    slots[s, h, i, j] = len(slots)
    return slots


SRC_SLOT = source_slots()


def line_sends(h, o):
    if o == 0:
        return [(1, 3), (-1, 1)]
    if o == 1 and VIA[h] == 1:
        return [(-1, 2)]
    if o == 3 and VIA[h] == -1:
        return [(1, 2)]
    return []


def line_up(h, o):
    if o == 2:
        return (1, 1) if VIA[h] == 1 else (-1, 3)
    return (1, 0) if o == 1 else (-1, 0)


class Here:
    def __init__(self):
        self.at = {a: lax.axis_index(a) for a in ROWS}
        self.step = 1 - 2 * self.at["c"]

    def next(self, axis, k=1):
        return {axis: lax.rem(self.at[axis] + RING + k * self.step, RING)}

    def sibling(self):
        return {"c": 1 - self.at["c"]}


def greet(peers):
    barrier = pltpu.get_barrier_semaphore()
    for peer in peers:
        pl.semaphore_signal(barrier, inc=1, device_id=peer, device_id_type=MESH)
    pl.semaphore_wait(barrier, len(peers))


def start_all(copies):
    for copy in copies:
        copy.start()
    return copies


def wait_all(copies):
    for copy in copies:
        copy.wait()


class Gather:
    def __init__(self, here, ref, order, sems):
        self.here, self.ref, self.order = here, ref, order
        self.ring_send, self.ring_recv, self.sib_send, self.sib_recv = sems
        self.sent = []

    def ring(self, h, src, dst, axis, way):
        n = piece_no(h, *dst)
        return pltpu.make_async_remote_copy(
            self.ref(0, h, *src), self.ref(0, h, *dst), self.ring_send.at[n], self.ring_recv.at[n],
            device_id=self.here.next(axis, way), device_id_type=MESH,
        )

    def sib(self, h, i, j):
        n = piece_no(h, i, j)
        return pltpu.make_async_remote_copy(
            self.ref(0, h, i, j), self.ref(1, h, i, j), self.sib_send.at[n], self.sib_recv.at[n],
            device_id=self.here.sibling(), device_id_type=MESH,
        )

    def spread(self, h, i, j):
        copies = []
        first, second = self.order[h]
        if j == 0:
            copies += [self.ring(h, (i, 0), (o, 0), first, way) for way, o in line_sends(h, i)]
        copies += [self.ring(h, (i, j), (i, o), second, way) for way, o in line_sends(h, j)]
        copies.append(self.sib(h, i, j))
        self.sent += start_all(copies)

    def spread_own(self):
        for h in range(GROUPS):
            self.spread(h, 0, 0)

    def relay(self, r, h):
        for i, j in ROUNDS[r]:
            self.ring(h, (0, 0), (i, j), "x", 1).wait_recv()
            self.spread(h, i, j)

    def arrive_sib(self, r):
        for h in range(GROUPS):
            for i, j in ROUNDS[r]:
                self.sib(h, i, j).wait_recv()

    def finish(self):
        for copy in self.sent:
            copy.wait_send()
        self.sent = []


def source_ref(src):
    def ref(*piece):
        return src.at[pl.ds(SRC_SLOT[piece] * SRC_PIECE, SRC_PIECE), :]

    return ref


def place_of(order, h, i, j):
    return (j, i) if order[h][0] == "x" else (i, j)


def target_ref(tgt, order):
    def ref(s, h, i, j):
        zd, xd = place_of(order, h, i, j)
        row = ((zd * 2 + s) * 8 + (h % 2) * 4 + xd) * TGT_PIECE
        return tgt.at[pl.ds(row, TGT_PIECE), pl.ds((h // 2) * 1024, 1024)]

    return ref


def unit_times(values, gain):
    scale = lax.rsqrt(jnp.mean(values * values, axis=-1, keepdims=True) + EPS)
    return values * scale * gain.astype(F32)


def whole_kernel(
    target, source, target_gain, source_gain, head_temp, final_gain, query_w, key_w, value_w, out_w,
    result,
    src, tgt, kv_w, q_w, kv_buf, q_buf, g_buf,
    w_buf, e_buf, o_buf, p_buf, att, att_out, ring_out, ring_in, st_own, st_in, hidden,
    s_ring_send, s_ring_recv, s_sib_send, s_sib_recv,
    t_ring_send, t_ring_recv, t_sib_send, t_sib_recv,
    load_sem, st_send, st_recv, sib_send, sib_recv, ring_send, ring_recv,
):
    here = Here()

    def projection_loads(layer):
        return [
            pltpu.make_async_copy(key_w.at[layer], kv_w.at[:, 0:512], load_sem.at[0]),
            pltpu.make_async_copy(value_w.at[layer], kv_w.at[:, 512:1024], load_sem.at[1]),
            pltpu.make_async_copy(query_w.at[layer], q_w, load_sem.at[2]),
        ]

    def out_load(layer):
        return pltpu.make_async_copy(out_w.at[layer], w_buf.at[0:1024], load_sem.at[3])

    def out_share(layer):
        return pltpu.make_async_remote_copy(
            out_w.at[layer], w_buf.at[1024:2048], sib_send.at[4], sib_recv.at[4],
            device_id=here.sibling(), device_id_type=MESH,
        )

    def place_target(values, layer):
        normed = unit_times(values, target_gain[layer : layer + 1, :]).astype(BF16)
        for half in range(2):
            tgt[half * 64 : half * 64 + 16, :] = normed[half * 16 : half * 16 + 16]

    def project_kv(start, rows, part):
        def body(n, carry):
            cols = pl.ds(pl.multiple_of(part * 512 + n * 256, 256), 256)
            kv = jnp.dot(src[start : start + rows, :], kv_w[:, cols], preferred_element_type=F32)
            kv_buf[start : start + rows, cols] = kv.astype(BF16)
            return carry

        lax.fori_loop(0, 2, body, 0)

    def project_q(o):
        def body(n, carry):
            cols = pl.ds(pl.multiple_of(n * 512, 512), 512)
            rows = pl.ds(pl.multiple_of(n * 256, 256), 256)
            q = jnp.dot(tgt[o * 256 : o * 256 + 256, :], q_w[:, cols], preferred_element_type=F32)
            q_buf[o, rows, :] = q.astype(BF16)
            return carry

        lax.fori_loop(0, 2, body, 0)

    def spread_ratio():
        ratio = source_gain[1:2, :].astype(F32) / source_gain[0:1, :].astype(F32)
        for k in range(D // 128):
            at = slice(k * 128, k * 128 + 128)
            g_buf[at, :] = jnp.broadcast_to(ratio[:, at], (128, 128)).T

    def fold_ratio():
        def body(k, carry):
            rows = pl.ds(pl.multiple_of(k * 128, 128), 128)
            g = jnp.concatenate([g_buf[rows, :]] * 4, axis=1)
            for n in range(2):
                cols = pl.ds(n * 512, 512)
                kv_w[rows, cols] = (kv_w[rows, cols].astype(F32) * g).astype(BF16)
            return carry

        lax.fori_loop(0, D // 128, body, 0)

    weights = start_all(projection_loads(0))
    out_own = out_load(0)
    out_own.start()
    normed = unit_times(source[...].astype(F32), source_gain[0:1, :]).astype(BF16)
    for h in range(GROUPS):
        row = SRC_SLOT[0, h, 0, 0] * SRC_PIECE
        src[row : row + 16, :] = normed[h * 16 : h * 16 + 16]
    place_target(target[...].astype(F32), 0)
    greet(
        [here.next(a, k) for a in "xyz" for k in (1, -1)] + [here.next("z", 2), here.sibling()]
    )
    sg = Gather(here, source_ref(src), XY, (s_ring_send, s_ring_recv, s_sib_send, s_sib_recv))
    tg = Gather(here, target_ref(tgt, XX), XX, (t_ring_send, t_ring_recv, t_sib_send, t_sib_recv))
    sg.spread_own()
    tg.spread_own()
    out_sib = out_share(0)
    out_sib.start()
    spread_ratio()
    wait_all(weights)
    for r in range(1, 5):
        for h in range(GROUPS):
            tg.relay(r, h)
            sg.relay(r, h)
            if h == 0:
                sg.arrive_sib(r - 1)
                tg.arrive_sib(r - 1)
            if r == 2 and h % 2 == 1:
                project_kv(0, 640, h // 2)
            if r == 3 and h == 0:
                project_kv(640, 384, 0)
            if r == 3 and h == 1:
                project_kv(640, 384, 1)
            if r == 3 and h == 2:
                project_kv(1024, 384, 0)
            if r == 3 and h == 3:
                project_kv(1024, 384, 1)
            if r == 4 and h == 0:
                project_q(0)
    project_q(1)
    project_q(3)
    tg.arrive_sib(4)
    project_q(2)
    sg.arrive_sib(4)
    project_kv(1408, 640, 0)
    project_kv(1408, 640, 1)
    sg.finish()
    tg.finish()

    for layer in range(2):
        attention_layer(
            layer, here, head_temp, q_buf, kv_buf, w_buf, e_buf, o_buf, p_buf, att, att_out,
            ring_out, ring_in, st_own, st_in, st_send, st_recv, sib_send, sib_recv, ring_send, ring_recv,
            target if layer == 0 else hidden, result if layer else hidden,
            final_gain if layer else None,
            lambda: start_all(projection_loads(1)) if layer == 0 else [],
            (lambda loads: (wait_all(loads), fold_ratio())) if layer == 0 else (lambda loads: None),
            [functools.partial(project_kv, n * 512, 512, part) for n in range(2) for part in range(2)] if layer == 0 else [],
            out_own, out_sib,
        )
        if layer == 1:
            break
        out_sib.wait_send()
        place_target(hidden[...], 1)
        out_own = out_load(1)
        out_own.start()
        tg = Gather(here, target_ref(tgt, XZ), XZ, (t_ring_send, t_ring_recv, t_sib_send, t_sib_recv))
        tg.spread_own()
        for r in range(1, 5):
            for h in range(GROUPS):
                tg.relay(r, h)
            tg.arrive_sib(r - 1)
            if r == 1:
                out_sib = out_share(1)
                out_sib.start()
            if r < 4:
                project_kv(1024 + 512 * ((r - 1) // 2), 512, (r - 1) % 2)
            if r == 3:
                project_q(0)
        project_kv(1536, 512, 1)
        project_q(1)
        project_q(3)
        tg.arrive_sib(4)
        project_q(2)
        tg.finish()
    out_sib.wait_send()


PAIR = {2: (0, 0), 1: (0, 1), 3: (1, 0), 0: (1, 1)}


def attention_layer(
    layer, here, head_temp, q_buf, kv_buf, w_buf, e_buf, o_buf, p_buf, att, att_out,
    ring_out, ring_in, st_own, st_in, st_send, st_recv, sib_send, sib_recv, ring_send, ring_recv,
    before, after, final_gain, start_loads, use_loads, fillers, out_own, out_sib,
):
    pending = []
    loads = start_loads()
    log2e = 1.0 / math.log(2.0)
    upper = lax.broadcasted_iota(jnp.int32, (512, 1), 0) < 256
    scale = jnp.where(upper, head_temp[layer, 0], head_temp[layer, 1]) * (HEAD_DIM ** (-0.5) * log2e)

    def stats_copy(k):
        return pltpu.make_async_remote_copy(
            st_own, st_in.at[k - 1], st_send.at[k - 1], st_recv.at[k - 1],
            device_id=here.next("z", k), device_id_type=MESH,
        )

    def score(o, carry):
        scores = lax.dot_general(
            q_buf[o], kv_buf[:, 0:512], (((1,), (1,)), ((), ())), preferred_element_type=F32
        )
        top = jnp.max(scores, axis=-1, keepdims=True)
        expo = jnp.exp2((scores - top) * scale)
        total = jnp.sum(expo, axis=-1, keepdims=True)
        e_buf[o] = expo.astype(BF16)
        lane = lax.broadcasted_iota(jnp.int32, (512, 128), 1)
        both = jnp.where(lane == 0, top * scale, total)
        st_own[o] = both.T[0:8, :]
        return carry

    def attend(o):
        return jnp.dot(e_buf[o], kv_buf[:, 512:1024], preferred_element_type=F32)

    def att_copy(o):
        pair, at = PAIR[o]
        return pltpu.make_async_remote_copy(
            att_out.at[o], att.at[pair, at * 128 : at * 128 + 128, 1024:2048], sib_send.at[o], sib_recv.at[o],
            device_id=here.sibling(), device_id_type=MESH,
        )

    def peer_stats(k, o, what):
        parts = []
        for n in range(4):
            there = (o + k) % RING if n % 2 == 0 else (o - k) % RING
            parts.append(st_in[k - 1, there, what : what + 1, n * 128 : n * 128 + 128])
        return jnp.concatenate(parts, axis=1)

    def weigh(o, values):
        own = st_own[o]
        tops = [own[0:1]] + [peer_stats(k, o, 0) for k in range(1, RING)]
        totals = [own[1:2]] + [peer_stats(k, o, 1) for k in range(1, RING)]
        top = functools.reduce(jnp.maximum, tops)
        total = sum(t * jnp.exp2(m - top) for m, t in zip(tops, totals))
        factor = jnp.exp2(own[0:1] - top) / total
        factor = jnp.broadcast_to(factor, (128, 512)).T
        factor = jnp.concatenate([factor] * 4, axis=1)
        rows = (values * factor).astype(BF16)
        pair, at = PAIR[o]
        for head in range(2):
            cols = slice(head * 512, head * 512 + 512)
            att_out[o, :, cols] = rows[head * 256 + 128 : head * 256 + 256]
            att[pair, at * 128 : at * 128 + 128, cols] = rows[head * 256 : head * 256 + 128]
        pending.extend(start_all([att_copy(o)]))

    def mix(pair):
        def body(n, carry):
            cols = pl.ds(pl.multiple_of(n * 512, 512), 512)
            p_buf[pair, :, cols] = jnp.dot(att[pair], w_buf[:, cols], preferred_element_type=F32)
            return carry

        lax.fori_loop(0, 4, body, 0)

    def ring_copy(h, i, j):
        axis, way = (XZ[h][1], line_up(h, j)[0]) if j else (XZ[h][0], line_up(h, i)[0])
        n = piece_no(h, i, j)
        return pltpu.make_async_remote_copy(
            ring_out.at[n], ring_in.at[n], ring_send.at[n], ring_recv.at[n],
            device_id=here.next(axis, way), device_id_type=MESH,
        )

    def below(h, i, j):
        labels = [(i, o) for way, o in line_sends(h, j)]
        if j == 0:
            labels += [(o, 0) for way, o in line_sends(h, i)]
        return labels

    def collect(h, i, j):
        zd, xd = place_of(XZ, h, i, j)
        pair, at = PAIR[zd]
        rows = pl.ds(at * 128 + ((h % 2) * 4 + xd) * 16, 16)
        value = p_buf[pair, rows, pl.ds((h // 2) * 1024, 1024)]
        for label in below(h, i, j):
            ring_copy(h, *label).wait_recv()
            value += ring_in[piece_no(h, *label)].astype(F32)
        return value

    def pass_on(h, i, j):
        ring_out[piece_no(h, i, j)] = collect(h, i, j).astype(BF16)
        pending.extend(start_all([ring_copy(h, i, j)]))

    passed = set()

    def pass_leaves(pair):
        for r in (4, 3, 2, 1):
            for h in range(GROUPS):
                for label in ROUNDS[r]:
                    zd, _ = place_of(XZ, h, *label)
                    if PAIR[zd][0] == pair and not below(h, *label):
                        pass_on(h, *label)
                        passed.add((h, label))

    lax.fori_loop(0, 4, score, 0)
    for k in range(1, RING):
        pending.extend(start_all([stats_copy(k)]))
    o_buf[0] = attend(2)
    o_buf[1] = attend(1)
    use_loads(loads)
    for k in range(1, RING):
        stats_copy(k).wait_recv()
    weigh(2, o_buf[0])
    weigh(1, o_buf[1])
    weigh(3, attend(3))
    weigh(0, attend(0))
    out_own.wait()
    out_sib.wait_recv()
    att_copy(2).wait_recv()
    att_copy(1).wait_recv()
    mix(0)
    pass_leaves(0)
    att_copy(3).wait_recv()
    att_copy(0).wait_recv()
    mix(1)
    pass_leaves(1)
    fillers = list(fillers)
    for r in (3, 2, 1):
        if fillers:
            fillers.pop(0)()
        for h in range(GROUPS):
            for label in ROUNDS[r]:
                if (h, label) not in passed:
                    pass_on(h, *label)
    for filler in fillers:
        filler()
    for half in range(2):
        at = slice(half * 16, half * 16 + 16)
        value = jnp.concatenate([collect(half, 0, 0), collect(half + 2, 0, 0)], axis=1)
        value += before[at, :].astype(F32)
        if final_gain is not None:
            value = unit_times(value, final_gain[...])
        after[at, :] = value
    for copy in pending:
        copy.wait_send()


def vmem(*shape, dtype=BF16):
    return pltpu.VMEM(shape, dtype)


ANY = pl.BlockSpec(memory_space=pl.ANY)
INV = pl.BlockSpec(memory_space=pltpu.VMEM)
DMA = pltpu.SemaphoreType.DMA


def per_device(
    target, source, target_gain, source_gain, query_w, key_w, value_w, out_w, head_temp, final_gain
):
    return pl.pallas_call(
        whole_kernel,
        out_shape=jax.ShapeDtypeStruct((32, D), F32),
        in_specs=[INV, INV, INV, INV, pl.BlockSpec(memory_space=pltpu.SMEM), INV, ANY, ANY, ANY, ANY],
        out_specs=INV,
        scratch_shapes=[
            vmem(2048, D), vmem(1024, D), vmem(D, 1024), vmem(D, 1024), vmem(2048, 1024), vmem(4, 512, HEAD_DIM),
            vmem(D, 128, dtype=F32),
            vmem(2048, D), vmem(4, 512, 2048), vmem(2, 512, HEAD_DIM, dtype=F32), vmem(2, 256, D, dtype=F32),
            vmem(2, 256, D), vmem(4, 128, 1024), vmem(64, 16, 1024), vmem(64, 16, 1024),
            vmem(4, 8, 512, dtype=F32), vmem(3, 4, 8, 512, dtype=F32), vmem(32, D, dtype=F32),
        ] + [DMA((64,))] * 8 + [DMA((4,)), DMA((3,)), DMA((3,)), DMA((5,)), DMA((5,)), DMA((64,)), DMA((64,))],
        compiler_params=pltpu.CompilerParams(
            collective_id=0, has_side_effects=True, vmem_limit_bytes=VMEM_LIMIT
        ),
        name="whole",
    )(target, source, target_gain, source_gain, head_temp, final_gain.reshape(1, D), query_w, key_w, value_w, out_w)


def solution(mesh):
    split = Mesh(mesh.devices.reshape(4, 4, 4, 2), ROWS)
    in_specs = (
        P(ROWS, None),
        P(ROWS, None),
        P(),
        P(),
        P(None, None, TP),
        P(None, None, TP),
        P(None, None, TP),
        P(None, TP, None),
        P(None, TP),
        P(),
    )
    return jax.shard_map(
        per_device, mesh=split, in_specs=in_specs, out_specs=P(ROWS, None), check_vma=False
    )
```

```python
import functools
import math

import jax
import jax.numpy as jnp
from jax import lax
from jax.experimental import pallas as pl
from jax.experimental.pallas import tpu as pltpu
from jax.sharding import Mesh
from jax.sharding import PartitionSpec as P

HEAD_DIM = 512
D = 2048
EPS = 1e-06
ROWS = ("z", "y", "x", "c")
TP = ("x", "c")
MESH = pl.DeviceIdType.MESH
RING = 4
BF16 = jnp.bfloat16
F32 = jnp.float32
GROUPS = 4
SRC_PIECE = 16
TGT_PIECE = 16
VMEM_LIMIT = 64 * 1024 * 1024 - 64 * 1024
VIA = (1, -1, -1, 1)
AWAY = (0, 1, 2, 1)
XX = (("x", "z"),) * GROUPS
XZ = (("x", "z"), ("z", "x")) * 2
XY = (("x", "y"), ("y", "x")) * 2
ROUNDS = [
    sorted(
        [(i, j) for i in range(RING) for j in range(RING) if AWAY[i] + AWAY[j] == r],
        key=lambda p: (p[1] != 0, p),
    )
    for r in range(5)
]


POS = {2: 0, 1: 1, 3: 2, 0: 3}


def piece_no(h, i, j):
    return h * 16 + i * 4 + j


def source_slots():
    slots = {}
    for pairs in ROUNDS:
        for s in range(2):
            for h in range(GROUPS):
                for i, j in pairs:
                    slots[s, h, i, j] = len(slots)
    return slots


SRC_SLOT = source_slots()


def line_sends(h, o):
    if o == 0:
        return [(1, 3), (-1, 1)]
    if o == 1 and VIA[h] == 1:
        return [(-1, 2)]
    if o == 3 and VIA[h] == -1:
        return [(1, 2)]
    return []


def line_up(h, o):
    if o == 2:
        return (1, 1) if VIA[h] == 1 else (-1, 3)
    return (1, 0) if o == 1 else (-1, 0)


def below(h, i, j):
    labels = [(i, o) for way, o in line_sends(h, j)]
    if j == 0:
        labels += [(o, 0) for way, o in line_sends(h, i)]
    return labels


JOINS = [
    (h, i, j) for h in range(GROUPS) for i in range(RING) for j in range(RING) if below(h, i, j)
]


class Here:
    def __init__(self):
        self.at = {a: lax.axis_index(a) for a in ROWS}
        self.step = 1 - 2 * self.at["c"]

    def next(self, axis, k=1):
        return {axis: lax.rem(self.at[axis] + RING + k * self.step, RING)}

    def sibling(self):
        return {"c": 1 - self.at["c"]}


def greet(peers):
    barrier = pltpu.get_barrier_semaphore()
    for peer in peers:
        pl.semaphore_signal(barrier, inc=1, device_id=peer, device_id_type=MESH)
    pl.semaphore_wait(barrier, len(peers))


def start_all(copies):
    for copy in copies:
        copy.start()
    return copies


def wait_all(copies):
    for copy in copies:
        copy.wait()


class Gather:
    def __init__(self, here, ref, bulk, order, sems, groups=tuple(range(GROUPS)), tag=0):
        self.here, self.ref, self.bulk, self.order = here, ref, bulk, order
        send, self.ring_recv, self.sib_recv = sems
        self.groups, self.tag, self.send = groups, tag, send.at[tag]
        self.sent = 0

    def ring(self, h, src, dst, axis, way):
        r = AWAY[dst[0]] + AWAY[dst[1]]
        return pltpu.make_async_remote_copy(
            self.ref(0, h, *src), self.ref(0, h, *dst), self.send, self.ring_recv.at[(r - 1) * GROUPS + h],
            device_id=self.here.next(axis, way), device_id_type=MESH,
        )

    def sib(self, h, i, j):
        return pltpu.make_async_remote_copy(
            self.ref(0, h, i, j), self.ref(1, h, i, j), self.send, self.sib_recv.at[self.tag * 5 + AWAY[i] + AWAY[j]],
            device_id=self.here.sibling(), device_id_type=MESH,
        )

    def whole(self, n, recv):
        return pltpu.make_async_remote_copy(
            self.bulk(n), self.bulk(n), self.send, recv,
            device_id=self.here.sibling(), device_id_type=MESH,
        )

    def spread(self, h, i, j):
        copies = []
        first, second = self.order[h]
        if j == 0:
            copies += [self.ring(h, (i, 0), (o, 0), first, way) for way, o in line_sends(h, i)]
        copies += [self.ring(h, (i, j), (i, o), second, way) for way, o in line_sends(h, j)]
        copies.append(self.sib(h, i, j))
        self.sent += len(start_all(copies))

    def spread_own(self):
        for h in self.groups:
            self.spread(h, 0, 0)

    def relay(self, r, h):
        self.whole(len(ROUNDS[r]), self.ring_recv.at[(r - 1) * GROUPS + h]).wait_recv()
        for i, j in ROUNDS[r]:
            self.spread(h, i, j)

    def arrive_sib(self, r):
        self.whole(len(ROUNDS[r]) * len(self.groups), self.sib_recv.at[self.tag * 5 + r]).wait_recv()

    def finish(self):
        self.whole(self.sent, self.sib_recv.at[0]).wait_send()
        self.sent = 0


def source_ref(src):
    def ref(*piece):
        return src.at[pl.ds(SRC_SLOT[piece] * SRC_PIECE, SRC_PIECE), :]

    return ref


def source_bulk(src):
    return lambda n: src.at[pl.ds(0, n * SRC_PIECE), :]


def place_of(order, h, i, j):
    return (j, i) if order[h][0] == "x" else (i, j)


def target_ref(tgt, order):
    def ref(s, h, i, j):
        zd, xd = place_of(order, h, i, j)
        row = (h % 2) * 512 + POS[zd] * 128 + s * 64 + xd * TGT_PIECE
        return tgt.at[pl.ds(row, TGT_PIECE), pl.ds((h // 2) * 1024, 1024)]

    return ref


def target_bulk(tgt):
    def bulk(n):
        if n <= 64:
            return tgt.at[pl.ds(0, n * TGT_PIECE), pl.ds(0, 1024)]
        return tgt.at[pl.ds(0, n * TGT_PIECE // 2), :]

    return bulk


def unit_times(values, gain):
    scale = lax.rsqrt(jnp.mean(values * values, axis=-1, keepdims=True) + EPS)
    return values * scale * gain.astype(F32)


def whole_kernel(
    target, source, target_gain, source_gain, head_temp, final_gain, query_w, key_w, value_w, out_w,
    result,
    src, tgt, kv_w, q_w, kv_buf, q_buf, g_buf,
    w_buf, e_buf, p_buf, att, att_out, ring_out, ring_in, st_own, st_in, hidden,
    s_send, s_ring_recv, s_sib_recv, t_send, t_ring_recv, t_sib_recv,
    load_sem, st_send, st_recv, sib_send, sib_recv, ring_send, ring_recv,
):
    here = Here()

    def projection_loads(layer):
        return [
            pltpu.make_async_copy(key_w.at[layer], kv_w.at[:, 0:512], load_sem.at[0]),
            pltpu.make_async_copy(value_w.at[layer], kv_w.at[:, 512:1024], load_sem.at[1]),
            pltpu.make_async_copy(query_w.at[layer], q_w, load_sem.at[2]),
        ]

    def out_load(layer):
        return pltpu.make_async_copy(out_w.at[layer], w_buf.at[0:1024], load_sem.at[3])

    def out_share(layer):
        return pltpu.make_async_remote_copy(
            out_w.at[layer], w_buf.at[1024:2048], sib_send.at[2], sib_recv.at[2],
            device_id=here.sibling(), device_id_type=MESH,
        )

    def place_target(values, layer, half):
        normed = unit_times(values, target_gain[layer : layer + 1, :]).astype(BF16)
        row = half * 512 + POS[0] * 128
        tgt[row : row + 16, :] = normed

    def project_kv(layer, start, rows, part):
        def body(n, carry):
            cols = pl.ds(pl.multiple_of(part * 512 + n * 256, 256), 256)
            kv = jnp.dot(src[start : start + rows, :], kv_w[:, cols], preferred_element_type=F32)
            kv_buf[layer, start : start + rows, cols] = kv.astype(BF16)
            return carry

        lax.fori_loop(0, 2, body, 0)

    def project_q(half, pair):
        start = half * 512 + pair * 256
        def body(head, carry):
            cols = pl.ds(pl.multiple_of(head * 512, 512), 512)
            q = jnp.dot(tgt[start : start + 256, :], q_w[:, cols], preferred_element_type=F32).astype(BF16)
            for n in range(4):
                rows = pl.ds(pl.multiple_of(n * 128 + head * 64, 64), 64)
                q_buf[half, pair, rows, :] = q[n * 64 : n * 64 + 64]
            return carry

        lax.fori_loop(0, 2, body, 0)

    def spread_ratio():
        ratio = source_gain[1:2, :].astype(F32) / source_gain[0:1, :].astype(F32)
        for k in range(D // 128):
            at = slice(k * 128, k * 128 + 128)
            g_buf[at, :] = jnp.broadcast_to(ratio[:, at], (128, 128)).T

    def fold_ratio():
        def body(k, carry):
            rows = pl.ds(pl.multiple_of(k * 128, 128), 128)
            g = jnp.concatenate([g_buf[rows, :]] * 4, axis=1)
            for n in range(2):
                cols = pl.ds(n * 512, 512)
                kv_w[rows, cols] = (kv_w[rows, cols].astype(F32) * g).astype(BF16)
            return carry

        lax.fori_loop(0, D // 128, body, 0)

    log2e = 1.0 / math.log(2.0)
    first_head = lax.rem(lax.broadcasted_iota(jnp.int32, (512, 1), 0), 128) < 64
    pending = ([], [])

    def stats_copy(half, k):
        return pltpu.make_async_remote_copy(
            st_own.at[half], st_in.at[k - 1, half], st_send.at[k - 1, half], st_recv.at[k - 1, half],
            device_id=here.next("z", k), device_id_type=MESH,
        )

    def score(layer, half, pair):
        scale = jnp.where(first_head, head_temp[layer, 0], head_temp[layer, 1]) * (HEAD_DIM ** (-0.5) * log2e)
        scores = lax.dot_general(
            q_buf[half, pair], kv_buf[layer, :, 0:512], (((1,), (1,)), ((), ())), preferred_element_type=F32
        )
        top = jnp.max(scores, axis=-1, keepdims=True)
        expo = jnp.exp2((scores - top) * scale)
        total = jnp.sum(expo, axis=-1, keepdims=True)
        e_buf[pair] = expo.astype(BF16)
        lane = lax.broadcasted_iota(jnp.int32, (512, 128), 1)
        both = jnp.where(lane == 0, top * scale, total)
        st_own[half, pair] = both.T[0:8, :]

    def send_stats(half):
        for k in range(1, RING):
            pending[half].extend(start_all([stats_copy(half, k)]))

    def wait_stats(half):
        for k in range(1, RING):
            stats_copy(half, k).wait_recv()

    def att_copy(half):
        return pltpu.make_async_remote_copy(
            att_out.at[half], att.at[half, :, 1024:2048], sib_send.at[half], sib_recv.at[half],
            device_id=here.sibling(), device_id_type=MESH,
        )

    def peer_stats(k, half, pair, what):
        parts = []
        for n in range(4):
            zd = ((2, 1), (3, 0))[pair][n // 2]
            at = POS[(zd + k) % RING if n % 2 == 0 else (zd - k) % RING]
            lanes = (at % 2) * 256 + (n % 2) * 128
            parts.append(st_in[k - 1, half, at // 2, what : what + 1, lanes : lanes + 128])
        return jnp.concatenate(parts, axis=1)

    def weigh(layer, half, pair):
        own = st_own[half, pair]
        tops = [own[0:1]] + [peer_stats(k, half, pair, 0) for k in range(1, RING)]
        totals = [own[1:2]] + [peer_stats(k, half, pair, 1) for k in range(1, RING)]
        top = functools.reduce(jnp.maximum, tops)
        total = sum(t * jnp.exp2(m - top) for m, t in zip(tops, totals))
        factor = jnp.exp2(own[0:1] - top) / total
        factor = jnp.broadcast_to(factor, (128, 512)).T
        factor = jnp.concatenate([factor] * 4, axis=1)
        values = jnp.dot(e_buf[pair], kv_buf[layer, :, 512:1024], preferred_element_type=F32)
        rows = (values * factor).astype(BF16)
        for n in range(4):
            at = slice((pair * 2 + n // 2) * 64, (pair * 2 + n // 2) * 64 + 64)
            for head in range(2):
                cols = slice(head * 512, head * 512 + 512)
                part = rows[n * 128 + head * 64 : n * 128 + head * 64 + 64]
                if n % 2 == 0:
                    att[half, at, cols] = part
                else:
                    att_out[half, at, cols] = part

    def send_att(half):
        pending[half].extend(start_all([att_copy(half)]))

    def mix(half):
        att_copy(half).wait_recv()

        def body(n, carry):
            cols = pl.ds(pl.multiple_of(n * 512, 512), 512)
            p_buf[half, :, cols] = jnp.dot(att[half], w_buf[:, cols], preferred_element_type=F32)
            return carry

        lax.fori_loop(0, 4, body, 0)

    def ring_copy(h, i, j):
        if j:
            way, up = line_up(h, j)
            axis, parent = XZ[h][1], (i, up)
        else:
            way, up = line_up(h, i)
            axis, parent = XZ[h][0], (up, 0)
        n = piece_no(h, i, j)
        return pltpu.make_async_remote_copy(
            ring_out.at[n], ring_in.at[n], ring_send.at[h % 2], ring_recv.at[JOINS.index((h, *parent))],
            device_id=here.next(axis, way), device_id_type=MESH,
        )

    def ring_bulk(half, n, recv):
        return pltpu.make_async_remote_copy(
            ring_out.at[0:n], ring_in.at[0:n], ring_send.at[half], recv,
            device_id=here.sibling(), device_id_type=MESH,
        )

    def collect(h, i, j):
        zd, xd = place_of(XZ, h, i, j)
        rows = pl.ds(POS[zd] * 64 + xd * 16, 16)
        value = p_buf[h % 2, rows, pl.ds((h // 2) * 1024, 1024)]
        labels = below(h, i, j)
        if labels:
            ring_bulk(h % 2, len(labels), ring_recv.at[JOINS.index((h, i, j))]).wait_recv()
        for label in labels:
            value += ring_in[piece_no(h, *label)].astype(F32)
        return value

    def pass_on(h, i, j):
        ring_out[piece_no(h, i, j)] = collect(h, i, j).astype(BF16)
        ring_copy(h, i, j).start()

    def reduce_leaves(half):
        for r in (4, 3, 2, 1):
            for h in (half, half + 2):
                for label in ROUNDS[r]:
                    if not below(h, *label):
                        pass_on(h, *label)

    def reduce_round(half, r):
        for h in (half, half + 2):
            for label in ROUNDS[r]:
                if below(h, *label):
                    pass_on(h, *label)

    def reduce_end(layer, half):
        at = slice(half * 16, half * 16 + 16)
        value = jnp.concatenate([collect(half, 0, 0), collect(half + 2, 0, 0)], axis=1)
        value += (hidden if layer else target)[at, :].astype(F32)
        ring_bulk(half, 30, ring_recv.at[0]).wait_send()
        for copy in pending[half]:
            copy.wait_send()
        pending[half].clear()
        if layer:
            result[at, :] = unit_times(value, final_gain[...][None, :])
        else:
            hidden[at, :] = value
            place_target(value, 1, half)

    def target_gathers(order):
        return [
            Gather(
                here, target_ref(tgt, order), target_bulk(tgt), order,
                (t_send, t_ring_recv, t_sib_recv), (half, half + 2), half,
            )
            for half in range(2)
        ]

    weights = start_all(projection_loads(0))
    out_own = out_load(0)
    out_own.start()
    normed = unit_times(source[...].astype(F32), source_gain[0:1, :]).astype(BF16)
    for h in range(GROUPS):
        row = SRC_SLOT[0, h, 0, 0] * SRC_PIECE
        src[row : row + 16, :] = normed[h * 16 : h * 16 + 16]
    for half in range(2):
        place_target(target[half * 16 : half * 16 + 16, :].astype(F32), 0, half)
    greet(
        [here.next(a, k) for a in "xyz" for k in (1, -1)] + [here.next("z", 2), here.sibling()]
    )
    sg = Gather(here, source_ref(src), source_bulk(src), XY, (s_send, s_ring_recv, s_sib_recv))
    tg = target_gathers(XX)
    sg.spread_own()
    for g in tg:
        g.spread_own()
    out_sib = out_share(0)
    out_sib.start()
    spread_ratio()
    wait_all(weights)
    for h in range(GROUPS):
        tg[h % 2].relay(1, h)
    for r in range(1, 5):
        for h in range(GROUPS):
            if r < 4:
                tg[h % 2].relay(r + 1, h)
            if r < 4 or h == 0:
                sg.relay(r, h)
            if h == 0:
                sg.arrive_sib(r - 1)
                for g in tg:
                    g.arrive_sib(r - 1)
            if r == 2 and h % 2 == 1:
                project_kv(0, 0, 640, h // 2)
            if r == 3:
                project_kv(0, 640 + 384 * (h // 2), 384, h % 2)
            if r == 4 and h == 0:
                project_q(0, 1)
    project_q(1, 1)
    for half in range(2):
        tg[half].arrive_sib(4)
        project_q(half, 0)
    for h in range(1, GROUPS):
        sg.relay(4, h)
    sg.arrive_sib(4)
    project_kv(0, 1408, 640, 0)
    project_kv(0, 1408, 640, 1)
    sg.finish()
    for g in tg:
        g.finish()

    loads = start_all(projection_loads(1))
    tg = target_gathers(XZ)
    blocks = [(start, part) for start in range(0, 2048, 512) for part in range(2)]

    def fill(n=1):
        for _ in range(n):
            start, part = blocks.pop(0)
            project_kv(1, start, 512, part)

    def score_pair(pair, carry):
        score(0, 0, pair)
        return carry

    lax.fori_loop(0, 2, score_pair, 0)
    send_stats(0)
    wait_all(loads)
    fold_ratio()
    wait_stats(0)
    weigh(0, 0, 0)
    weigh(0, 0, 1)
    send_att(0)
    out_own.wait()
    out_sib.wait()
    fill(2)
    mix(0)
    reduce_leaves(0)
    score(0, 1, 0)
    reduce_round(0, 3)
    score(0, 1, 1)
    send_stats(1)
    reduce_round(0, 2)
    fill()
    reduce_round(0, 1)
    wait_stats(1)
    weigh(0, 1, 0)
    reduce_end(0, 0)
    tg[0].spread_own()
    weigh(0, 1, 1)
    send_att(1)
    fill()
    relay = lambda half, r: [tg[half].relay(r, h) for h in (half, half + 2)]
    relay(0, 1)
    mix(1)
    reduce_leaves(1)
    out_own = out_load(1)
    out_own.start()
    relay(0, 2)
    fill()
    reduce_round(1, 3)
    relay(0, 3)
    fill()
    reduce_round(1, 2)
    relay(0, 4)
    fill()
    reduce_round(1, 1)
    for r in range(4):
        tg[0].arrive_sib(r)
    project_q(0, 1)
    reduce_end(0, 1)
    tg[1].spread_own()
    tg[0].arrive_sib(4)
    project_q(0, 0)
    relay(1, 1)
    fill()
    tg[1].arrive_sib(0)
    out_sib = out_share(1)
    out_sib.start()
    score(1, 0, 0)
    relay(1, 2)
    score(1, 0, 1)
    send_stats(0)
    relay(1, 3)
    tg[1].arrive_sib(1)
    tg[1].arrive_sib(2)
    relay(1, 4)
    tg[1].arrive_sib(3)
    project_q(1, 1)
    wait_stats(0)
    weigh(1, 0, 0)
    weigh(1, 0, 1)
    send_att(0)
    tg[1].arrive_sib(4)
    project_q(1, 0)
    out_own.wait()
    out_sib.wait()
    mix(0)
    reduce_leaves(0)
    score(1, 1, 0)
    reduce_round(0, 3)
    score(1, 1, 1)
    send_stats(1)
    reduce_round(0, 2)
    reduce_round(0, 1)
    wait_stats(1)
    weigh(1, 1, 0)
    weigh(1, 1, 1)
    send_att(1)
    reduce_end(1, 0)
    mix(1)
    reduce_leaves(1)
    for r in (3, 2, 1):
        reduce_round(1, r)
    reduce_end(1, 1)
    for g in tg:
        g.finish()


def vmem(*shape, dtype=BF16):
    return pltpu.VMEM(shape, dtype)


ANY = pl.BlockSpec(memory_space=pl.ANY)
INV = pl.BlockSpec(memory_space=pltpu.VMEM)
DMA = pltpu.SemaphoreType.DMA


def per_device(
    target, source, target_gain, source_gain, query_w, key_w, value_w, out_w, head_temp, final_gain
):
    return pl.pallas_call(
        whole_kernel,
        out_shape=jax.ShapeDtypeStruct((32, D), F32),
        in_specs=[INV, INV, INV, INV, pl.BlockSpec(memory_space=pltpu.SMEM), INV, ANY, ANY, ANY, ANY],
        out_specs=INV,
        scratch_shapes=[
            vmem(2048, D), vmem(1024, D), vmem(D, 1024), vmem(D, 1024), vmem(2, 2048, 1024),
            vmem(2, 2, 512, HEAD_DIM), vmem(D, 128, dtype=F32),
            vmem(2048, D), vmem(2, 512, 2048), vmem(2, 256, D, dtype=F32),
            vmem(2, 256, D), vmem(2, 256, 1024), vmem(64, 16, 1024), vmem(64, 16, 1024),
            vmem(2, 2, 8, 512, dtype=F32), vmem(3, 2, 2, 8, 512, dtype=F32), vmem(32, D, dtype=F32),
            DMA((1,)), DMA((16,)), DMA((5,)), DMA((2,)), DMA((16,)), DMA((10,)),
            DMA((4,)), DMA((3, 2)), DMA((3, 2)), DMA((3,)), DMA((3,)), DMA((2,)), DMA((len(JOINS),)),
        ],
        compiler_params=pltpu.CompilerParams(
            collective_id=0, has_side_effects=True, vmem_limit_bytes=VMEM_LIMIT
        ),
        name="whole",
    )(target, source, target_gain, source_gain, head_temp, final_gain, query_w, key_w, value_w, out_w)


def solution(mesh):
    split = Mesh(mesh.devices.reshape(4, 4, 4, 2), ROWS)
    in_specs = (
        P(ROWS, None),
        P(ROWS, None),
        P(),
        P(),
        P(None, None, TP),
        P(None, None, TP),
        P(None, None, TP),
        P(None, TP, None),
        P(None, TP),
        P(),
    )
    return jax.shard_map(
        per_device, mesh=split, in_specs=in_specs, out_specs=P(ROWS, None), check_vma=False
    )
```

```python
import functools
import math

import jax
import jax.numpy as jnp
from jax import lax
from jax.experimental import pallas as pl
from jax.experimental.pallas import tpu as pltpu
from jax.sharding import Mesh
from jax.sharding import PartitionSpec as P

HEAD_DIM = 512
D = 2048
EPS = 1e-06
ROWS = ("z", "y", "x", "c")
TP = ("x", "c")
MESH = pl.DeviceIdType.MESH
RING = 4
BF16 = jnp.bfloat16
F32 = jnp.float32
GROUPS = 4
SRC_PIECE = 16
TGT_PIECE = 16
VMEM_LIMIT = 64 * 1024 * 1024 - 64 * 1024
VIA = (1, -1, -1, 1)
AWAY = (0, 1, 2, 1)
XX = (("x", "z"),) * GROUPS
XZ = (("x", "z"), ("z", "x")) * 2
XY = (("x", "y"), ("y", "x")) * 2
ROUNDS = [
    sorted(
        [(i, j) for i in range(RING) for j in range(RING) if AWAY[i] + AWAY[j] == r],
        key=lambda p: (p[1] != 0, p),
    )
    for r in range(5)
]


def piece_no(h, i, j):
    return h * 16 + i * 4 + j


def source_slots():
    slots = {}
    for pairs in ROUNDS:
        for s in range(2):
            for h in range(GROUPS):
                for i, j in pairs:
                    slots[s, h, i, j] = len(slots)
    return slots


SRC_SLOT = source_slots()


def line_sends(h, o):
    if o == 0:
        return [(1, 3), (-1, 1)]
    if o == 1 and VIA[h] == 1:
        return [(-1, 2)]
    if o == 3 and VIA[h] == -1:
        return [(1, 2)]
    return []


def line_up(h, o):
    if o == 2:
        return (1, 1) if VIA[h] == 1 else (-1, 3)
    return (1, 0) if o == 1 else (-1, 0)


def below(h, i, j):
    labels = [(i, o) for way, o in line_sends(h, j)]
    if j == 0:
        labels += [(o, 0) for way, o in line_sends(h, i)]
    return labels


JOINS = [
    (h, i, j) for h in range(GROUPS) for i in range(RING) for j in range(RING) if below(h, i, j)
]


class Here:
    def __init__(self):
        self.at = {a: lax.axis_index(a) for a in ROWS}
        self.step = 1 - 2 * self.at["c"]

    def next(self, axis, k=1):
        return {axis: lax.rem(self.at[axis] + RING + k * self.step, RING)}

    def sibling(self):
        return {"c": 1 - self.at["c"]}


def greet(peers):
    barrier = pltpu.get_barrier_semaphore()
    for peer in peers:
        pl.semaphore_signal(barrier, inc=1, device_id=peer, device_id_type=MESH)
    pl.semaphore_wait(barrier, len(peers))


def start_all(copies):
    for copy in copies:
        copy.start()
    return copies


def wait_all(copies):
    for copy in copies:
        copy.wait()


class Gather:
    def __init__(self, here, ref, bulk, order, sems):
        self.here, self.ref, self.bulk, self.order = here, ref, bulk, order
        self.send, self.ring_recv, self.sib_recv = sems
        self.sent = 0

    def ring(self, h, src, dst, axis, way):
        r = AWAY[dst[0]] + AWAY[dst[1]]
        return pltpu.make_async_remote_copy(
            self.ref(0, h, *src), self.ref(0, h, *dst), self.send.at[0], self.ring_recv.at[(r - 1) * GROUPS + h],
            device_id=self.here.next(axis, way), device_id_type=MESH,
        )

    def sib(self, h, i, j):
        return pltpu.make_async_remote_copy(
            self.ref(0, h, i, j), self.ref(1, h, i, j), self.send.at[0], self.sib_recv.at[AWAY[i] + AWAY[j]],
            device_id=self.here.sibling(), device_id_type=MESH,
        )

    def whole(self, n, recv):
        return pltpu.make_async_remote_copy(
            self.bulk(n), self.bulk(n), self.send.at[0], recv,
            device_id=self.here.sibling(), device_id_type=MESH,
        )

    def spread(self, h, i, j):
        copies = []
        first, second = self.order[h]
        if j == 0:
            copies += [self.ring(h, (i, 0), (o, 0), first, way) for way, o in line_sends(h, i)]
        copies += [self.ring(h, (i, j), (i, o), second, way) for way, o in line_sends(h, j)]
        copies.append(self.sib(h, i, j))
        self.sent += len(start_all(copies))

    def spread_own(self):
        for h in range(GROUPS):
            self.spread(h, 0, 0)

    def relay(self, r, h):
        self.whole(len(ROUNDS[r]), self.ring_recv.at[(r - 1) * GROUPS + h]).wait_recv()
        for i, j in ROUNDS[r]:
            self.spread(h, i, j)

    def arrive_sib(self, r):
        self.whole(len(ROUNDS[r]) * GROUPS, self.sib_recv.at[r]).wait_recv()

    def finish(self):
        self.whole(self.sent, self.sib_recv.at[0]).wait_send()
        self.sent = 0


def source_ref(src):
    def ref(*piece):
        return src.at[pl.ds(SRC_SLOT[piece] * SRC_PIECE, SRC_PIECE), :]

    return ref


def source_bulk(src):
    return lambda n: src.at[pl.ds(0, n * SRC_PIECE), :]


def place_of(order, h, i, j):
    return (j, i) if order[h][0] == "x" else (i, j)


def target_ref(tgt, order):
    def ref(s, h, i, j):
        zd, xd = place_of(order, h, i, j)
        row = ((zd * 2 + s) * 8 + (h % 2) * 4 + xd) * TGT_PIECE
        return tgt.at[pl.ds(row, TGT_PIECE), pl.ds((h // 2) * 1024, 1024)]

    return ref


def target_bulk(tgt):
    def bulk(n):
        if n <= 64:
            return tgt.at[pl.ds(0, n * TGT_PIECE), pl.ds(0, 1024)]
        return tgt.at[pl.ds(0, n * TGT_PIECE // 2), :]

    return bulk


def unit_times(values, gain):
    scale = lax.rsqrt(jnp.mean(values * values, axis=-1, keepdims=True) + EPS)
    return values * scale * gain.astype(F32)


def whole_kernel(
    target, source, target_gain, source_gain, head_temp, final_gain, query_w, key_w, value_w, out_w,
    result,
    src, tgt, kv_w, q_w, kv_buf, q_buf, g_buf,
    w_buf, e_buf, o_buf, p_buf, att, att_out, ring_out, ring_in, st_own, st_in, hidden,
    s_send, s_ring_recv, s_sib_recv, t_send, t_ring_recv, t_sib_recv,
    load_sem, st_send, st_recv, sib_send, sib_recv, ring_send, ring_recv,
):
    here = Here()

    def projection_loads(layer):
        return [
            pltpu.make_async_copy(key_w.at[layer], kv_w.at[:, 0:512], load_sem.at[0]),
            pltpu.make_async_copy(value_w.at[layer], kv_w.at[:, 512:1024], load_sem.at[1]),
            pltpu.make_async_copy(query_w.at[layer], q_w, load_sem.at[2]),
        ]

    def out_load(layer):
        return pltpu.make_async_copy(out_w.at[layer], w_buf.at[0:1024], load_sem.at[3])

    def out_share(layer):
        return pltpu.make_async_remote_copy(
            out_w.at[layer], w_buf.at[1024:2048], sib_send.at[4], sib_recv.at[4],
            device_id=here.sibling(), device_id_type=MESH,
        )

    def place_target(values, layer):
        normed = unit_times(values, target_gain[layer : layer + 1, :]).astype(BF16)
        for half in range(2):
            tgt[half * 64 : half * 64 + 16, :] = normed[half * 16 : half * 16 + 16]

    def project_kv(start, rows, part):
        def body(n, carry):
            cols = pl.ds(pl.multiple_of(part * 512 + n * 256, 256), 256)
            kv = jnp.dot(src[start : start + rows, :], kv_w[:, cols], preferred_element_type=F32)
            kv_buf[start : start + rows, cols] = kv.astype(BF16)
            return carry

        lax.fori_loop(0, 2, body, 0)

    def project_q(o):
        def body(n, carry):
            cols = pl.ds(pl.multiple_of(n * 512, 512), 512)
            rows = pl.ds(pl.multiple_of(n * 256, 256), 256)
            q = jnp.dot(tgt[o * 256 : o * 256 + 256, :], q_w[:, cols], preferred_element_type=F32)
            q_buf[o, rows, :] = q.astype(BF16)
            return carry

        lax.fori_loop(0, 2, body, 0)

    def spread_ratio():
        ratio = source_gain[1:2, :].astype(F32) / source_gain[0:1, :].astype(F32)
        for k in range(D // 128):
            at = slice(k * 128, k * 128 + 128)
            g_buf[at, :] = jnp.broadcast_to(ratio[:, at], (128, 128)).T

    def fold_ratio():
        def body(k, carry):
            rows = pl.ds(pl.multiple_of(k * 128, 128), 128)
            g = jnp.concatenate([g_buf[rows, :]] * 4, axis=1)
            for n in range(2):
                cols = pl.ds(n * 512, 512)
                kv_w[rows, cols] = (kv_w[rows, cols].astype(F32) * g).astype(BF16)
            return carry

        lax.fori_loop(0, D // 128, body, 0)

    weights = start_all(projection_loads(0))
    out_own = out_load(0)
    out_own.start()
    normed = unit_times(source[...].astype(F32), source_gain[0:1, :]).astype(BF16)
    for h in range(GROUPS):
        row = SRC_SLOT[0, h, 0, 0] * SRC_PIECE
        src[row : row + 16, :] = normed[h * 16 : h * 16 + 16]
    place_target(target[...].astype(F32), 0)
    greet(
        [here.next(a, k) for a in "xyz" for k in (1, -1)] + [here.next("z", 2), here.sibling()]
    )
    sg = Gather(here, source_ref(src), source_bulk(src), XY, (s_send, s_ring_recv, s_sib_recv))
    tg = Gather(here, target_ref(tgt, XX), target_bulk(tgt), XX, (t_send, t_ring_recv, t_sib_recv))
    sg.spread_own()
    tg.spread_own()
    out_sib = out_share(0)
    out_sib.start()
    spread_ratio()
    wait_all(weights)
    for h in range(GROUPS):
        tg.relay(1, h)
    for r in range(1, 5):
        for h in range(GROUPS):
            if r < 4:
                tg.relay(r + 1, h)
            if r < 4 or h == 0:
                sg.relay(r, h)
            if h == 0:
                sg.arrive_sib(r - 1)
                tg.arrive_sib(r - 1)
            if r == 2 and h % 2 == 1:
                project_kv(0, 640, h // 2)
            if r == 3:
                project_kv(640 + 384 * (h // 2), 384, h % 2)
            if r == 4 and h == 0:
                project_q(0)
    project_q(1)
    project_q(3)
    tg.arrive_sib(4)
    project_q(2)
    for h in range(1, GROUPS):
        sg.relay(4, h)
    sg.arrive_sib(4)
    project_kv(1408, 640, 0)
    project_kv(1408, 640, 1)
    sg.finish()
    tg.finish()

    for layer in range(2):
        attention_layer(
            layer, here, head_temp, q_buf, kv_buf, w_buf, e_buf, o_buf, p_buf, att, att_out,
            ring_out, ring_in, st_own, st_in, st_send, st_recv, sib_send, sib_recv, ring_send, ring_recv,
            target if layer == 0 else hidden, result if layer else hidden,
            final_gain if layer else None,
            lambda: start_all(projection_loads(1)) if layer == 0 else [],
            (lambda loads: (wait_all(loads), fold_ratio())) if layer == 0 else (lambda loads: None),
            [functools.partial(project_kv, n * 512, 512, part) for n in range(2) for part in range(2)] if layer == 0 else [],
            out_own, out_sib,
        )
        if layer == 1:
            break
        out_sib.wait_send()
        place_target(hidden[...], 1)
        out_own = out_load(1)
        out_own.start()
        tg = Gather(here, target_ref(tgt, XZ), target_bulk(tgt), XZ, (t_send, t_ring_recv, t_sib_recv))
        tg.spread_own()
        for r in range(1, 5):
            for h in range(GROUPS):
                tg.relay(r, h)
            tg.arrive_sib(r - 1)
            if r == 1:
                out_sib = out_share(1)
                out_sib.start()
            if r < 4:
                project_kv(1024 + 512 * ((r - 1) // 2), 512, (r - 1) % 2)
            if r == 3:
                project_q(0)
        project_kv(1536, 512, 1)
        project_q(1)
        project_q(3)
        tg.arrive_sib(4)
        project_q(2)
        tg.finish()
    out_sib.wait_send()


PAIR = {2: (0, 0), 1: (0, 1), 3: (1, 0), 0: (1, 1)}


def attention_layer(
    layer, here, head_temp, q_buf, kv_buf, w_buf, e_buf, o_buf, p_buf, att, att_out,
    ring_out, ring_in, st_own, st_in, st_send, st_recv, sib_send, sib_recv, ring_send, ring_recv,
    before, after, final_gain, start_loads, use_loads, fillers, out_own, out_sib,
):
    pending = []
    loads = start_loads()
    log2e = 1.0 / math.log(2.0)
    upper = lax.broadcasted_iota(jnp.int32, (512, 1), 0) < 256
    scale = jnp.where(upper, head_temp[layer, 0], head_temp[layer, 1]) * (HEAD_DIM ** (-0.5) * log2e)

    def stats_copy(k):
        return pltpu.make_async_remote_copy(
            st_own, st_in.at[k - 1], st_send.at[k - 1], st_recv.at[k - 1],
            device_id=here.next("z", k), device_id_type=MESH,
        )

    def score(o, carry):
        scores = lax.dot_general(
            q_buf[o], kv_buf[:, 0:512], (((1,), (1,)), ((), ())), preferred_element_type=F32
        )
        top = jnp.max(scores, axis=-1, keepdims=True)
        expo = jnp.exp2((scores - top) * scale)
        total = jnp.sum(expo, axis=-1, keepdims=True)
        e_buf[o] = expo.astype(BF16)
        lane = lax.broadcasted_iota(jnp.int32, (512, 128), 1)
        both = jnp.where(lane == 0, top * scale, total)
        st_own[o] = both.T[0:8, :]
        return carry

    def attend(o):
        return jnp.dot(e_buf[o], kv_buf[:, 512:1024], preferred_element_type=F32)

    def att_copy(o):
        pair, at = PAIR[o]
        return pltpu.make_async_remote_copy(
            att_out.at[o], att.at[pair, at * 128 : at * 128 + 128, 1024:2048], sib_send.at[o], sib_recv.at[o],
            device_id=here.sibling(), device_id_type=MESH,
        )

    def peer_stats(k, o, what):
        parts = []
        for n in range(4):
            there = (o + k) % RING if n % 2 == 0 else (o - k) % RING
            parts.append(st_in[k - 1, there, what : what + 1, n * 128 : n * 128 + 128])
        return jnp.concatenate(parts, axis=1)

    def weigh(o, values):
        own = st_own[o]
        tops = [own[0:1]] + [peer_stats(k, o, 0) for k in range(1, RING)]
        totals = [own[1:2]] + [peer_stats(k, o, 1) for k in range(1, RING)]
        top = functools.reduce(jnp.maximum, tops)
        total = sum(t * jnp.exp2(m - top) for m, t in zip(tops, totals))
        factor = jnp.exp2(own[0:1] - top) / total
        factor = jnp.broadcast_to(factor, (128, 512)).T
        factor = jnp.concatenate([factor] * 4, axis=1)
        rows = (values * factor).astype(BF16)
        pair, at = PAIR[o]
        for head in range(2):
            cols = slice(head * 512, head * 512 + 512)
            att_out[o, :, cols] = rows[head * 256 + 128 : head * 256 + 256]
            att[pair, at * 128 : at * 128 + 128, cols] = rows[head * 256 : head * 256 + 128]
        pending.extend(start_all([att_copy(o)]))

    def mix(pair):
        def body(n, carry):
            cols = pl.ds(pl.multiple_of(n * 512, 512), 512)
            p_buf[pair, :, cols] = jnp.dot(att[pair], w_buf[:, cols], preferred_element_type=F32)
            return carry

        lax.fori_loop(0, 4, body, 0)

    def ring_copy(h, i, j):
        if j:
            way, up = line_up(h, j)
            axis, parent = XZ[h][1], (i, up)
        else:
            way, up = line_up(h, i)
            axis, parent = XZ[h][0], (up, 0)
        n = piece_no(h, i, j)
        return pltpu.make_async_remote_copy(
            ring_out.at[n], ring_in.at[n], ring_send.at[0], ring_recv.at[JOINS.index((h, *parent))],
            device_id=here.next(axis, way), device_id_type=MESH,
        )

    def ring_bulk(n, recv):
        return pltpu.make_async_remote_copy(
            ring_out.at[0:n], ring_in.at[0:n], ring_send.at[0], recv,
            device_id=here.sibling(), device_id_type=MESH,
        )

    def collect(h, i, j):
        zd, xd = place_of(XZ, h, i, j)
        pair, at = PAIR[zd]
        rows = pl.ds(at * 128 + ((h % 2) * 4 + xd) * 16, 16)
        value = p_buf[pair, rows, pl.ds((h // 2) * 1024, 1024)]
        labels = below(h, i, j)
        if labels:
            ring_bulk(len(labels), ring_recv.at[JOINS.index((h, i, j))]).wait_recv()
        for label in labels:
            value += ring_in[piece_no(h, *label)].astype(F32)
        return value

    def pass_on(h, i, j):
        ring_out[piece_no(h, i, j)] = collect(h, i, j).astype(BF16)
        ring_copy(h, i, j).start()

    passed = set()

    def pass_leaves(pair):
        for r in (4, 3, 2, 1):
            for h in range(GROUPS):
                for label in ROUNDS[r]:
                    zd, _ = place_of(XZ, h, *label)
                    if PAIR[zd][0] == pair and not below(h, *label):
                        pass_on(h, *label)
                        passed.add((h, label))

    lax.fori_loop(0, 4, score, 0)
    for k in range(1, RING):
        pending.extend(start_all([stats_copy(k)]))
    o_buf[0] = attend(2)
    o_buf[1] = attend(1)
    use_loads(loads)
    for k in range(1, RING):
        stats_copy(k).wait_recv()
    weigh(2, o_buf[0])
    weigh(1, o_buf[1])
    weigh(3, attend(3))
    weigh(0, attend(0))
    out_own.wait()
    out_sib.wait_recv()
    att_copy(2).wait_recv()
    att_copy(1).wait_recv()
    mix(0)
    pass_leaves(0)
    att_copy(3).wait_recv()
    att_copy(0).wait_recv()
    mix(1)
    pass_leaves(1)
    fillers = list(fillers)
    for r in (3, 2, 1):
        if fillers:
            fillers.pop(0)()
        for h in range(GROUPS):
            for label in ROUNDS[r]:
                if (h, label) not in passed:
                    pass_on(h, *label)
    for filler in fillers:
        filler()
    for half in range(2):
        at = slice(half * 16, half * 16 + 16)
        value = jnp.concatenate([collect(half, 0, 0), collect(half + 2, 0, 0)], axis=1)
        value += before[at, :].astype(F32)
        if final_gain is not None:
            value = unit_times(value, final_gain[...][None, :])
        after[at, :] = value
    for copy in pending:
        copy.wait_send()
    ring_bulk(15 * GROUPS, ring_recv.at[0]).wait_send()


def vmem(*shape, dtype=BF16):
    return pltpu.VMEM(shape, dtype)


ANY = pl.BlockSpec(memory_space=pl.ANY)
INV = pl.BlockSpec(memory_space=pltpu.VMEM)
DMA = pltpu.SemaphoreType.DMA


def per_device(
    target, source, target_gain, source_gain, query_w, key_w, value_w, out_w, head_temp, final_gain
):
    return pl.pallas_call(
        whole_kernel,
        out_shape=jax.ShapeDtypeStruct((32, D), F32),
        in_specs=[INV, INV, INV, INV, pl.BlockSpec(memory_space=pltpu.SMEM), INV, ANY, ANY, ANY, ANY],
        out_specs=INV,
        scratch_shapes=[
            vmem(2048, D), vmem(1024, D), vmem(D, 1024), vmem(D, 1024), vmem(2048, 1024), vmem(4, 512, HEAD_DIM),
            vmem(D, 128, dtype=F32),
            vmem(2048, D), vmem(4, 512, 2048), vmem(2, 512, HEAD_DIM, dtype=F32), vmem(2, 256, D, dtype=F32),
            vmem(2, 256, D), vmem(4, 128, 1024), vmem(64, 16, 1024), vmem(64, 16, 1024),
            vmem(4, 8, 512, dtype=F32), vmem(3, 4, 8, 512, dtype=F32), vmem(32, D, dtype=F32),
        ] + [DMA((1,)), DMA((16,)), DMA((5,))] * 2 + [
            DMA((4,)), DMA((3,)), DMA((3,)), DMA((5,)), DMA((5,)), DMA((1,)), DMA((len(JOINS),)),
        ],
        compiler_params=pltpu.CompilerParams(
            collective_id=0, has_side_effects=True, vmem_limit_bytes=VMEM_LIMIT
        ),
        name="whole",
    )(target, source, target_gain, source_gain, head_temp, final_gain, query_w, key_w, value_w, out_w)


def solution(mesh):
    split = Mesh(mesh.devices.reshape(4, 4, 4, 2), ROWS)
    in_specs = (
        P(ROWS, None),
        P(ROWS, None),
        P(),
        P(),
        P(None, None, TP),
        P(None, None, TP),
        P(None, None, TP),
        P(None, TP, None),
        P(None, TP),
        P(),
    )
    return jax.shard_map(
        per_device, mesh=split, in_specs=in_specs, out_specs=P(ROWS, None), check_vma=False
    )
```
